32 devices in a mesh: sp: 8 (over z, y), tp: 4 (over x, core).
Axes of the slice: x: 2, y: 2, z: 4, core: 2. Of those that a mesh axis runs over, the one named last changes fastest.
Arguments:
- tokens: bfloat16 [2048, 4096], P(('sp', 'tp')), may hold values from -700 to 700
- down_query: bfloat16 [4096, 1024], replicated, may hold values from -0.09375 to 0.09375
- down_latent: bfloat16 [4096, 512], replicated, may hold values from -0.09375 to 0.09375
- down_rotary: bfloat16 [4096, 64], replicated, may hold values from -0.09375 to 0.09375
- query_gain: float32 [1024], replicated, may hold values from 0.1 to 1.9
- latent_gain: float32 [512], replicated, may hold values from 0.1 to 1.9
- up_query: bfloat16 [1024, 2048], P(None, 'tp'), may hold values from -0.1875 to 0.1875
- up_query_rotary: bfloat16 [1024, 1024], P(None, 'tp'), may hold values from -0.1875 to 0.1875
- up_key: bfloat16 [512, 2048], P(None, 'tp'), may hold values from -0.25 to 0.25
- up_value: bfloat16 [512, 2048], P(None, 'tp'), may hold values from -0.25 to 0.25
- out_weight: bfloat16 [2048, 4096], P('tp'), may hold values from -0.39648438 to 0.39648438
Outputs:
- mixed: bfloat16 [2048, 4096], P(('sp', 'tp'))
The draws below stay inside these ranges and needn't reach their ends.
All inputs are finite; a program needn't handle non-finite values.
Results may differ from the reference program's by a relative error of at most 0.03.
Values may be sent and summed in bfloat16 or wider, within the bound.
A program may use at most 192 MiB of HBM per device.

```python
import jax
import jax.numpy as jnp
from jax import lax

D = 4096
HEADS = 16
NOPE = 128
ROPE = 64
VDIM = 128
QRANK = 1024
KVRANK = 512
TOK_DEV = 256
TOKENS = 2048
N_TP = 4


def draw_tokens(key, part):
    first_key, second_key, third_key = jax.random.split(jax.random.fold_in(key, 11), 3)
    offsets = jax.random.normal(second_key, (TOKENS // TOK_DEV, D), jnp.float32) * 0.7
    shifted = jnp.repeat(offsets, TOK_DEV, axis=0)
    rough = jax.random.normal(first_key, (TOKENS, D), jnp.float32) + shifted
    return jnp.clip(rough, -700.0, 700.0).astype(jnp.bfloat16)


def shard_levels(stream_key, dims, cuts, smallest, high):
    loudness, own = 1.0, jax.random.fold_in(stream_key, 6)
    for dim, parts in cuts:
        heights = jnp.exp(jax.random.uniform(jax.random.fold_in(own, dim), (parts,), jnp.float32, smallest / len(cuts), high / len(cuts)))
        loudness = loudness * jnp.repeat(heights, dims[dim] // parts).reshape([-1 if axis == dim else 1 for axis in range(len(dims))])
    return loudness


def normal_values(rng, shape, width, bound, pieces=(), held_as=jnp.bfloat16):
    values = jax.random.normal(rng, shape, jnp.float32) * width
    if len(pieces) > 0:
        values = shard_levels(rng, shape, pieces, -0.22, 0.18) * values
    return jnp.clip(values, min=-bound, max=bound).astype(held_as)


def setup_inputs(seed: int = 0) -> dict:
    splits = jax.random.split(jax.random.key(seed), 12)
    tokens = draw_tokens(jax.random.fold_in(splits[11], 71), 0)
    down_query = normal_values(splits[1], (D, QRANK), D ** -0.5, 0.09375)
    down_latent = normal_values(splits[2], (D, KVRANK), D ** -0.5, 0.09375)
    down_rotary = normal_values(splits[3], (D, ROPE), D ** -0.5, 0.09375)
    query_gain = jnp.clip(1.0 + 0.18 * jax.random.normal(splits[4], (QRANK,), jnp.float32), 0.1, 1.9)
    latent_gain = jnp.clip(1.0 + 0.18 * jax.random.normal(splits[5], (KVRANK,), jnp.float32), 0.1, 1.9)
    up_query = normal_values(splits[6], (QRANK, HEADS * NOPE), QRANK ** -0.5, 0.1875, ((1, 4),))
    up_query_rotary = normal_values(splits[7], (QRANK, HEADS * ROPE), QRANK ** -0.5, 0.1875, ((1, 4),))
    up_key = normal_values(splits[8], (KVRANK, HEADS * NOPE), KVRANK ** -0.5, 0.25, ((1, 4),))
    up_value = normal_values(splits[9], (KVRANK, HEADS * VDIM), KVRANK ** -0.5, 0.25, ((1, 4),))
    out_weight = normal_values(splits[10], (HEADS * VDIM, D), (3.0 * (HEADS * VDIM) ** -0.5), 0.39648438, ((0, 4),))
    return dict(tokens=tokens, down_query=down_query, down_latent=down_latent, down_rotary=down_rotary, query_gain=query_gain, latent_gain=latent_gain, up_query=up_query, up_query_rotary=up_query_rotary, up_key=up_key, up_value=up_value, out_weight=out_weight)


rope_base = 500000.0
norm_eps = 1e-06
masked_score = -1e+30

def rotate_half(values, positions):
    half = values.shape[-1] // 2
    inverse = rope_base ** (-jnp.arange(0, 2 * half, 2, dtype=jnp.float32) / (2 * half))
    angles = positions.astype(jnp.float32)[:, None] * inverse
    if values.ndim == 3:
        angles = angles[:, None, :]
    cosine = jnp.cos(angles)
    sine = jnp.sin(angles)
    first = values[..., :half]
    second = values[..., half:]
    return jnp.concatenate([first * cosine - second * sine, second * cosine + first * sine], axis=-1)

def norm_rows(values, gain):
    return values * lax.rsqrt(lax.optimization_barrier(jnp.mean(values * values, axis=-1, keepdims=True)) + norm_eps) * gain

def reference(tokens, down_query, down_latent, down_rotary, query_gain, latent_gain, up_query, up_query_rotary, up_key, up_value, out_weight):
    positions = jnp.arange(TOKENS, dtype=jnp.int32)
    query_latent = norm_rows(jnp.dot(tokens, down_query, preferred_element_type=jnp.float32), query_gain).astype(jnp.bfloat16)
    kv_latent = norm_rows(jnp.dot(tokens, down_latent, preferred_element_type=jnp.float32), latent_gain).astype(jnp.bfloat16)
    key_rotary = rotate_half(jnp.dot(tokens, down_rotary, preferred_element_type=jnp.float32), positions).astype(jnp.bfloat16)
    query_plain = jnp.dot(query_latent, up_query, preferred_element_type=jnp.float32).astype(jnp.bfloat16).reshape(TOKENS, HEADS, NOPE)
    query_turned = rotate_half(jnp.dot(query_latent, up_query_rotary, preferred_element_type=jnp.float32).reshape(TOKENS, HEADS, ROPE), positions).astype(jnp.bfloat16)
    key_plain = jnp.dot(kv_latent, up_key, preferred_element_type=jnp.float32).astype(jnp.bfloat16).reshape(TOKENS, HEADS, NOPE)
    values = jnp.dot(kv_latent, up_value, preferred_element_type=jnp.float32).astype(jnp.bfloat16).reshape(TOKENS, HEADS, VDIM)
    factor = (NOPE + ROPE) ** (-0.5)
    block = 512 if TOKENS % 512 == 0 else TOKENS
    outputs = []
    for first in range(0, TOKENS, block):
        stop = first + block
        scores = jnp.einsum('qhd,khd->hqk', query_plain[first:stop].astype(jnp.float32), key_plain[:stop].astype(jnp.float32))
        scores = scores + jnp.einsum('qhr,kr->hqk', query_turned[first:stop].astype(jnp.float32), key_rotary[:stop].astype(jnp.float32))
        scores = scores * factor
        allowed = (positions[:stop][None, :] <= positions[first:stop][:, None])[None]
        scores = jnp.where(allowed, scores, masked_score)
        best = lax.optimization_barrier(jnp.max(scores, axis=-1, keepdims=True))
        weights = jnp.where(allowed, jnp.exp(scores - best), 0.0)
        total = lax.optimization_barrier(jnp.sum(weights, axis=-1))
        rounded = lax.optimization_barrier(weights.astype(jnp.bfloat16)).astype(jnp.float32)
        summed = jnp.einsum('hqk,khd->qhd', rounded, values[:stop].astype(jnp.float32))
        outputs.append((summed / jnp.transpose(total)[:, :, None]).astype(jnp.bfloat16).reshape(block, HEADS * VDIM))
    attended = jnp.concatenate(outputs, axis=0)
    group_width = HEADS * VDIM // N_TP
    mixed = jnp.zeros((TOKENS, D), jnp.float32)
    for group in range(N_TP):
        lower = group * group_width
        partial_sum = jnp.dot(attended[:, lower:lower + group_width], out_weight[lower:lower + group_width], preferred_element_type=jnp.float32)
        mixed = mixed + lax.optimization_barrier(partial_sum.astype(jnp.bfloat16)).astype(jnp.float32)
    return mixed.astype(jnp.bfloat16)
```

```python
import functools

import jax
import jax.numpy as jnp
import numpy as np
from jax import lax
from jax.experimental import pallas as pl
from jax.experimental.pallas import tpu as pltpu
from jax.sharding import PartitionSpec as P

NOPE = 128
ROPE = 64
HALF = ROPE // 2
VDIM = 128
LANES = 128

rope_base = 500000.0
norm_eps = 1e-06
masked_score = -1e30
log2e = 1.4426950408889634

MESH = pl.DeviceIdType.MESH
F32 = jnp.float32
BF16 = jnp.bfloat16


def dot(a, b):
    return jnp.dot(a, b, preferred_element_type=F32)


def dot_nt(a, b):
    return lax.dot_general(a, b, (((1,), (1,)), ((), ())), preferred_element_type=F32)


def normed(v, gain):
    return v * lax.rsqrt(jnp.mean(v * v, axis=-1, keepdims=True) + norm_eps) * gain


def kernel(
    S,
    T,
    chunks,
    pieces,
    tokens_hbm,
    dq_hbm,
    dl_hbm,
    dr_hbm,
    qg_hbm,
    lg_hbm,
    uq_hbm,
    ur_hbm,
    uk_hbm,
    uv_hbm,
    ow_hbm,
    kbase_hbm,
    kstep_hbm,
    qbase_hbm,
    qstep_hbm,
    out_ref,
    tokens,
    dq,
    dl,
    dr,
    qg,
    lg,
    uq,
    ur,
    uk,
    uv,
    ow,
    kbase,
    kstep,
    qbase,
    qstep,
    kv,
    ql,
    qt,
    acc,
    best,
    att,
    pair_out,
    pair_in,
    kept,
    cross_out,
    cross_in,
    uqt,
    urt,
    uvt,
    keys,
    vals,
    rots,
    load_sem,
    kv_send,
    kv_recv,
    q_send,
    q_recv,
    pair_send,
    pair_recv,
    cross_send,
    cross_recv,
):
    O = S // 2
    rows = tokens.shape[0]
    span = rows * T
    depth = tokens.shape[1]
    heads = qt.shape[0]
    rank = dl.shape[1]
    slabs = rank // LANES
    sp = lax.axis_index("sp")
    tp = lax.axis_index("tp")
    o, i = sp // 2, sp % 2
    g, c = tp // 2, tp % 2

    def dev(o_, i_, g_, c_):
        return {"sp": o_ * 2 + i_, "tp": g_ * 2 + c_}

    across = dev(o, i, 1 - g, c)
    beside = dev(o, 1 - i, g, c)
    mate = dev(o, i, g, 1 - c)

    barrier = pltpu.get_barrier_semaphore()
    for d in range(1, O):
        pl.semaphore_signal(barrier, inc=1, device_id=dev((o + d) % O, i, g, c), device_id_type=MESH)
    for target in (across, beside, mate):
        pl.semaphore_signal(barrier, inc=1, device_id=target, device_id_type=MESH)

    step = depth // chunks
    loads = []

    def load(src, dst):
        copy = pltpu.make_async_copy(src, dst, load_sem.at[len(loads)])
        loads.append(copy)
        copy.start()
        return copy

    tok_load = load(tokens_hbm, tokens)
    dr_load = load(dr_hbm, dr)
    dl_loads = [load(dl_hbm.at[pl.ds(k * step, step)], dl.at[pl.ds(k * step, step)]) for k in range(chunks)]
    key_loads = [load(lg_hbm, lg), load(kbase_hbm.at[sp * T + tp], kbase), load(kstep_hbm, kstep)]
    dq_loads = [load(dq_hbm.at[pl.ds(k * step, step)], dq.at[pl.ds(k * step, step)]) for k in range(chunks)]
    qg_load = load(qg_hbm, qg)
    up_loads = [load(uv_hbm, uv), load(uq_hbm, uq), load(ur_hbm, ur)]
    uk_load = load(uk_hbm, uk)
    table_loads = [load(qbase_hbm.at[sp], qbase), load(qstep_hbm, qstep)]
    ow_load = load(ow_hbm, ow)

    def block(o_, i_, g_, c_):
        return (o_ * 2 + i_) * T + g_ * 2 + c_

    def block_rows(b):
        return pl.ds(pl.multiple_of(b * rows, rows), rows)

    def kv_copy(b, target, index):
        part = kv.at[b]
        return pltpu.make_async_remote_copy(
            src_ref=part,
            dst_ref=part,
            send_sem=kv_send.at[index],
            recv_sem=kv_recv.at[b],
            device_id=target,
            device_id_type=MESH,
        )

    def kv_wait(b):
        kv_copy(b, mate, 0).wait_recv()

    lane = lax.broadcasted_iota(jnp.int32, (rows, LANES), 1)

    tok_load.wait()
    dr_load.wait()
    turned = dot_nt(tokens[...], dr[...])
    latent = jnp.zeros((rows, rank), F32)
    for k in range(chunks):
        dl_loads[k].wait()
        latent += dot(tokens[:, k * step : (k + 1) * step], dl[k * step : (k + 1) * step, :])
    for copy in key_loads:
        copy.wait()
    start_cos, start_sin = kbase[0:1, :], kbase[8:9, :]
    cosine = start_cos * kstep[:rows, :] - start_sin * kstep[rows:, :]
    sine = start_sin * kstep[:rows, :] + start_cos * kstep[rows:, :]
    turned = jnp.concatenate([turned, jnp.zeros((rows, LANES - ROPE), F32)], axis=1)
    low = lane % ROPE < HALF
    swapped = jnp.where(low, -pltpu.roll(turned, LANES - HALF, 1), pltpu.roll(turned, HALF, 1))
    turned = turned * cosine + swapped * sine
    packed = jnp.where(lane[: rows // 2] < ROPE, turned[: rows // 2], pltpu.roll(turned[rows // 2 :], ROPE, 1))
    mine = block(o, i, g, c)
    latent = normed(latent, lg[...]).astype(BF16)
    for k in range(slabs):
        kv[mine, k * rows : (k + 1) * rows, :] = latent[:, k * LANES : (k + 1) * LANES]
    kv[mine, slabs * rows :, :] = packed.astype(BF16)

    pl.semaphore_wait(barrier, O - 1 + 3)

    def start(copy):
        copy.start()

    def sent(copy):
        copy.wait_send()

    def up(b, first, act):
        for d in reversed(range(1, O)):

            @pl.when(o + d < O)
            def _(d=d):
                act(kv_copy(b, dev((o + d) % O, i, g, c), first + d))

    def relay_column(d, act):
        b = block(o - d, i, g, c)
        act(kv_copy(b, across, O + d))

        @pl.when((i == 0) | (d > 0))
        def _():
            act(kv_copy(b, beside, 2 * O + d))

        act(kv_copy(b, mate, 4 * O + 4 * d))

    def relay_across(d, act):
        b = block(o - d, i, 1 - g, c)

        @pl.when((d == 0) & ((i == 0) | (o < O - 1)))
        def _():
            act(kv_copy(b, beside, 0))

        act(kv_copy(b, mate, 4 * O + 4 * d + 1))

    def relay_beside(d, act):
        act(kv_copy(block(o - d, 1 - i, g, c), mate, 4 * O + 4 * d + 2))

    def relay_corner(d, act):
        b = block(o - d, 1 - i, 1 - g, c)

        @pl.when((i == 1) | (d > 0))
        def _():
            act(kv_copy(b, mate, 4 * O + 4 * d + 3))

    def column_in(d):
        kv_wait(block(o - d, i, g, c))
        relay_column(d, start)

    def across_in(d):
        kv_wait(block(o - d, i, 1 - g, c))
        relay_across(d, start)

    def beside_in(d):
        kv_wait(block(o - d, 1 - i, g, c))
        relay_beside(d, start)

    def corner_in(d):
        kv_wait(block(o - d, 1 - i, 1 - g, c))
        relay_corner(d, start)

    def each(first, last, body):
        def run(d, carry):
            body(d)
            return carry

        lax.fori_loop(first, last, run, 0)

    up(mine, 0, start)
    relay_column(0, start)

    query = jnp.zeros((rows, dq.shape[1]), F32)
    for k in range(chunks):
        dq_loads[k].wait()
        query += dot(tokens[:, k * step : (k + 1) * step], dq[k * step : (k + 1) * step, :])
    qg_load.wait()
    own_rows = pl.ds(pl.multiple_of(tp * rows, rows), rows)
    ql[own_rows, :] = normed(query, qg[...]).astype(BF16)

    def q_copy(t, target, index):
        part = ql.at[block_rows(t)]
        return pltpu.make_async_remote_copy(
            src_ref=part,
            dst_ref=part,
            send_sem=q_send.at[index],
            recv_sem=q_recv.at[t],
            device_id=target,
            device_id_type=MESH,
        )

    other = (1 - g) * 2 + c
    q_copies = [q_copy(tp, across, 0), q_copy(tp, mate, 1), q_copy(other, mate, 2)]
    q_copies[0].start()
    q_copies[1].start()

    for copy in up_loads:
        copy.wait()
    uk_load.wait()
    uvt[...] = uv[...].T

    def latents(s):
        return jnp.concatenate(
            [
                jnp.concatenate([kv[s * T + t, k * rows : (k + 1) * rows, :] for k in range(slabs)], axis=1)
                for t in range(T)
            ],
            axis=0,
        )

    def rotaries(s):
        parts = []
        for t in range(T):
            both = kv[s * T + t, slabs * rows :, :].astype(F32)
            parts += [both, pltpu.roll(both, ROPE, 1)]
        return jnp.concatenate(parts, axis=0).astype(BF16)

    wide = 2 * LANES

    def head_parts(s, slot):
        lat = latents(s)

        def key_part(n):
            keys[slot, :, n : n + wide] = dot(lat, uk[:, n : n + wide]).astype(BF16)

        def value_part(n):
            vals[slot, n : n + wide, :] = dot_nt(uvt[n : n + wide, :], lat).astype(BF16)

        def rotary_part():
            rots[slot] = rotaries(s)

        parts = [functools.partial(key_part, n) for n in range(0, heads * NOPE, wide)]
        parts += [functools.partial(value_part, n) for n in range(0, heads * VDIM, wide)]
        return [rotary_part] + parts

    def kv_heads(s, slot):
        for part in head_parts(s, slot):
            part()

    across_in(0)
    pl.when(o >= 1)(lambda: column_in(1))
    pl.when(i == 1)(lambda: beside_in(0))
    uqt[...] = uq[...].T
    urt[...] = ur[...].T
    kv_wait(block(o, i, g, 1 - c))
    kv_wait(block(o, i, 1 - g, 1 - c))
    kv_heads(sp, 0)
    each(2, o + 1, column_in)

    @pl.when((i == 1) | (o < O - 1))
    def _():
        corner_in(0)
        up(block(o, 1 - i, 1 - g, c), 3 * O, start)

    q_copy(other, mate, 2).wait_recv()
    q_copies[2].start()
    for copy in table_loads:
        copy.wait()
    q_cos = jnp.concatenate([qbase[:HALF, :]] * (span // LANES), axis=1)
    q_sin = jnp.concatenate([qbase[HALF:, :]] * (span // LANES), axis=1)
    step_cos, step_sin = qstep[:HALF, :], qstep[HALF:, :]
    q_cos, q_sin = q_cos * step_cos - q_sin * step_sin, q_sin * step_cos + q_cos * step_sin
    q_copy(g * 2 + 1 - c, mate, 0).wait_recv()
    q_copy((1 - g) * 2 + 1 - c, mate, 0).wait_recv()

    scale = (NOPE + ROPE) ** (-0.5) * log2e
    plain = dot_nt(uqt[...], ql[...]) * scale
    turning = dot_nt(urt[...], ql[...]) * scale
    for h in range(heads):
        qt[h, :NOPE, :] = plain[h * NOPE : (h + 1) * NOPE, :].astype(BF16)
        first = turning[h * ROPE : h * ROPE + HALF, :]
        second = turning[h * ROPE + HALF : (h + 1) * ROPE, :]
        qt[h, NOPE : NOPE + HALF, :] = (first * q_cos - second * q_sin).astype(BF16)
        qt[h, NOPE + HALF : NOPE + ROPE, :] = (second * q_cos + first * q_sin).astype(BF16)
        qt[h, NOPE + ROPE :, :] = jnp.zeros((LANES - ROPE, span), BF16)

    def attend(slot, first=False, ahead=None):
        rot = rots[slot]
        ones = jnp.ones((acc.shape[1] - VDIM, span), BF16)
        parts = [] if ahead is None else head_parts(*ahead)
        if first:
            k_pos = lax.broadcasted_iota(jnp.int32, (span, span), 0)
            q_pos = lax.broadcasted_iota(jnp.int32, (span, span), 1)
            allowed = k_pos <= q_pos

        def score(h):
            key = jnp.concatenate([keys[slot, :, h * NOPE : (h + 1) * NOPE], rot], axis=1)
            return dot(key, qt[h])

        later = score(0)
        for h in range(heads):
            scores = later
            if h + 1 < heads:
                later = score(h + 1)
            for part in parts[h::heads]:
                part()
            value = jnp.concatenate([vals[slot, h * VDIM : (h + 1) * VDIM, :], ones], axis=0)
            if first:
                scores = jnp.where(allowed, scores, masked_score)
            new = jnp.max(scores, axis=0, keepdims=True)
            if not first:
                old = best[h][:1]
                new = jnp.maximum(old, new)
            weights = jnp.exp2(scores - new).astype(BF16)
            if first:
                acc[h] = dot(value, weights)
            else:
                acc[h] = acc[h] * jnp.exp2(old - new) + dot(value, weights)
            best[h] = jnp.broadcast_to(new, best.shape[1:])

    def relay_in(s):
        d, same = o - s // 2, s % 2 == i
        pl.when((d > 0) & same)(lambda: across_in(d))

        @pl.when((d > 0) & jnp.logical_not(same))
        def _():
            beside_in(d)
            corner_in(d)

    def mate_in(s):
        kv_wait(s * T + g * 2 + 1 - c)
        kv_wait(s * T + (1 - g) * 2 + 1 - c)

    attend(0, first=True)

    @pl.when(sp >= 1)
    def _():
        relay_in(sp - 1)
        pl.when(sp >= 2)(lambda: relay_in(sp - 2))
        mate_in(sp - 1)
        kv_heads(sp - 1, 1)

        def both(j):
            pl.when(sp - j >= 2)(lambda: relay_in(sp - j - 2))
            mate_in(sp - j - 1)
            attend(j % 2, ahead=(sp - j - 1, (j + 1) % 2))

        each(1, sp, both)
        attend(sp % 2)

    for h in range(heads):
        whole = acc[h]
        att[:, h * VDIM : (h + 1) * VDIM] = (whole[:VDIM] / whole[VDIM : VDIM + 1]).T.astype(BF16)

    ow_load.wait()
    width = ow.shape[1] // pieces
    lag = min(3, pieces)

    def pair_copy(phase, j):
        return pltpu.make_async_remote_copy(
            src_ref=pair_out.at[phase, j],
            dst_ref=pair_in.at[phase, j],
            send_sem=pair_send.at[phase * pieces + j],
            recv_sem=pair_recv.at[phase * pieces + j],
            device_id=mate,
            device_id_type=MESH,
        )

    def cross_copy(j):
        return pltpu.make_async_remote_copy(
            src_ref=cross_out.at[j],
            dst_ref=cross_in.at[j],
            send_sem=cross_send.at[j],
            recv_sem=cross_recv.at[j],
            device_id=across,
            device_id_type=MESH,
        )

    def project(phase, group, j):
        top = att[block_rows(group * 2 + 1 - c), :]
        low_part = att[block_rows(group * 2 + c), :]
        part = dot(jnp.concatenate([top, low_part], axis=0), ow[:, j * width : (j + 1) * width])
        pair_out[phase, j] = part[:rows].astype(BF16)
        kept[phase, j] = part[rows:]
        pair_copy(phase, j).start()

    def cross(j):
        pair_copy(0, j).wait_recv()
        cross_out[j] = (kept[0, j] + pair_in[0, j].astype(F32)).astype(BF16)
        cross_copy(j).start()

    for j in range(pieces):
        project(0, 1 - g, j)
        if j >= lag:
            cross(j - lag)
    for j in range(pieces - lag, pieces):
        cross(j)
    for j in range(pieces):
        project(1, g, j)

    up(mine, 0, sent)

    def drain(d):
        relay_column(d, sent)
        relay_across(d, sent)

        @pl.when((i == 1) | (d > 0))
        def _():
            relay_beside(d, sent)

        relay_corner(d, sent)

    each(0, o + 1, drain)
    pl.when((i == 1) | (o < O - 1))(lambda: up(block(o, 1 - i, 1 - g, c), 3 * O, sent))
    for copy in q_copies:
        copy.wait_send()

    for j in range(pieces):
        pair_copy(1, j).wait_recv()
        cross_copy(j).wait_recv()
        total = kept[1, j] + pair_in[1, j].astype(F32) + cross_in[j].astype(F32)
        out_ref[:, j * width : (j + 1) * width] = total.astype(BF16)

    for j in range(pieces):
        pair_copy(0, j).wait_send()
        pair_copy(1, j).wait_send()
        cross_copy(j).wait_send()


def solution(mesh):
    S, T = mesh.shape["sp"], mesh.shape["tp"]
    assert S % 2 == 0 and T == 4

    def local(tokens, dq, dl, dr, qg, lg, uq, ur, uk, uv, ow):
        rows, depth = tokens.shape
        span = rows * T
        heads = uk.shape[1] // NOPE
        width = ow.shape[1]
        rank = dl.shape[1]
        chunks, pieces = 4, 8
        inverse = np.float32(rope_base) ** (-np.arange(0, ROPE, 2, dtype=np.float32) / np.float32(ROPE))
        inverse = inverse.astype(np.float64)
        tiled = np.tile(inverse, LANES // HALF)

        def both(angles, axis):
            return np.concatenate([np.cos(angles), np.sin(angles)], axis=axis)

        key_base = np.repeat((np.arange(S * T) * rows)[:, None, None] * tiled, 8, axis=1)
        key_step = np.arange(rows)[:, None] * tiled
        query_base = np.repeat((np.arange(S) * span)[:, None, None] * inverse[:, None], LANES, axis=2)
        query_step = inverse[:, None] * np.arange(span)
        tables = [
            jnp.asarray(a, F32) for a in (both(key_base, 1), both(key_step, 0), both(query_base, 1), both(query_step, 0))
        ]
        O = S // 2
        hbm = pl.BlockSpec(memory_space=pl.ANY)
        vmem = pl.BlockSpec(memory_space=pltpu.VMEM)
        dma = lambda n: pltpu.SemaphoreType.DMA((n,))
        like = lambda a: pltpu.VMEM(a.shape, a.dtype)
        operands = [tokens, dq, dl, dr.T, qg.reshape(1, -1), lg.reshape(1, -1), uq, ur, uk, uv, ow, *tables]
        operands = [pltpu.with_memory_space_constraint(a, pltpu.HBM) for a in operands]
        block_height = rows * rank // LANES + rows // 2
        return pl.pallas_call(
            functools.partial(kernel, S, T, chunks, pieces),
            out_shape=jax.ShapeDtypeStruct((rows, width), BF16),
            in_specs=[hbm] * len(operands),
            out_specs=vmem,
            scratch_shapes=[
                *[like(a) for a in operands[:11]],
                pltpu.VMEM((16, LANES), F32),
                pltpu.VMEM((2 * rows, LANES), F32),
                pltpu.VMEM((ROPE, LANES), F32),
                pltpu.VMEM((ROPE, span), F32),
                pltpu.VMEM((S * T, block_height, LANES), BF16),
                pltpu.VMEM((span, dq.shape[1]), BF16),
                pltpu.VMEM((heads, NOPE + LANES, span), BF16),
                pltpu.VMEM((heads, VDIM + 16, span), F32),
                pltpu.VMEM((heads, 8, span), F32),
                pltpu.VMEM((span, heads * VDIM), BF16),
                pltpu.VMEM((2, pieces, rows, width // pieces), BF16),
                pltpu.VMEM((2, pieces, rows, width // pieces), BF16),
                pltpu.VMEM((2, pieces, rows, width // pieces), F32),
                pltpu.VMEM((pieces, rows, width // pieces), BF16),
                pltpu.VMEM((pieces, rows, width // pieces), BF16),
                pltpu.VMEM(uq.shape[::-1], BF16),
                pltpu.VMEM(ur.shape[::-1], BF16),
                pltpu.VMEM(uv.shape[::-1], BF16),
                pltpu.VMEM((2, span, heads * NOPE), BF16),
                pltpu.VMEM((2, heads * VDIM, span), BF16),
                pltpu.VMEM((2, span, LANES), BF16),
                dma(2 * chunks + 13),
                dma(8 * O),
                dma(S * T),
                dma(3),
                dma(T),
                dma(2 * pieces),
                dma(2 * pieces),
                dma(pieces),
                dma(pieces),
            ],
            compiler_params=pltpu.CompilerParams(
                collective_id=0, has_side_effects=True, vmem_limit_bytes=54 * 1024 * 1024
            ),
        )(*operands)

    return jax.shard_map(
        local,
        mesh=mesh,
        in_specs=(
            P(("sp", "tp"), None),
            P(),
            P(),
            P(),
            P(),
            P(),
            P(None, "tp"),
            P(None, "tp"),
            P(None, "tp"),
            P(None, "tp"),
            P("tp", None),
        ),
        out_specs=P(("sp", "tp"), None),
        check_vma=False,
    )
```

```python
import functools

import jax
import jax.numpy as jnp
import numpy as np
from jax import lax
from jax.experimental import pallas as pl
from jax.experimental.pallas import tpu as pltpu
from jax.sharding import PartitionSpec as P

NOPE = 128
ROPE = 64
HALF = ROPE // 2
VDIM = 128
LANES = 128

rope_base = 500000.0
norm_eps = 1e-06
masked_score = -1e30
log2e = 1.4426950408889634

MESH = pl.DeviceIdType.MESH
F32 = jnp.float32
BF16 = jnp.bfloat16


def dot(a, b):
    return jnp.dot(a, b, preferred_element_type=F32)


def dot_nt(a, b):
    return lax.dot_general(a, b, (((1,), (1,)), ((), ())), preferred_element_type=F32)


def normed(v, gain):
    return v * lax.rsqrt(jnp.mean(v * v, axis=-1, keepdims=True) + norm_eps) * gain


def kernel(
    S,
    T,
    chunks,
    pieces,
    tokens_hbm,
    dq_hbm,
    dl_hbm,
    dr_hbm,
    qg_hbm,
    lg_hbm,
    uq_hbm,
    ur_hbm,
    uk_hbm,
    uv_hbm,
    ow_hbm,
    kbase_hbm,
    kstep_hbm,
    qbase_hbm,
    qstep_hbm,
    out_ref,
    tokens,
    dq,
    dl,
    dr,
    qg,
    lg,
    uq,
    ur,
    uk,
    uv,
    ow,
    kbase,
    kstep,
    qbase,
    qstep,
    kv,
    ql,
    qt,
    acc,
    best,
    att,
    pair_out,
    pair_in,
    kept,
    cross_out,
    cross_in,
    uqt,
    urt,
    uvt,
    keys,
    vals,
    rots,
    scored,
    load_sem,
    kv_send,
    kv_recv,
    q_send,
    q_recv,
    pair_send,
    pair_recv,
    cross_send,
    cross_recv,
):
    O = S // 2
    rows = tokens.shape[0]
    span = rows * T
    depth = tokens.shape[1]
    heads = qt.shape[1]
    rank = dl.shape[1]
    slabs = rank // LANES
    sp = lax.axis_index("sp")
    tp = lax.axis_index("tp")
    o, i = sp // 2, sp % 2
    g, c = tp // 2, tp % 2

    def dev(o_, i_, g_, c_):
        return {"sp": o_ * 2 + i_, "tp": g_ * 2 + c_}

    across = dev(o, i, 1 - g, c)
    beside = dev(o, 1 - i, g, c)
    mate = dev(o, i, g, 1 - c)

    barrier = pltpu.get_barrier_semaphore()
    for d in range(1, O):
        pl.semaphore_signal(barrier, inc=1, device_id=dev((o + d) % O, i, g, c), device_id_type=MESH)
    for target in (across, beside, mate):
        pl.semaphore_signal(barrier, inc=1, device_id=target, device_id_type=MESH)

    step = depth // chunks
    loads = []

    def load(src, dst):
        copy = pltpu.make_async_copy(src, dst, load_sem.at[len(loads)])
        loads.append(copy)
        copy.start()
        return copy

    tok_load = load(tokens_hbm, tokens)
    dr_load = load(dr_hbm, dr)
    dl_loads = [load(dl_hbm.at[pl.ds(k * step, step)], dl.at[pl.ds(k * step, step)]) for k in range(chunks)]
    key_loads = [load(lg_hbm, lg), load(kbase_hbm.at[sp * T + tp], kbase), load(kstep_hbm, kstep)]
    dq_loads = [load(dq_hbm.at[pl.ds(k * step, step)], dq.at[pl.ds(k * step, step)]) for k in range(chunks)]
    qg_load = load(qg_hbm, qg)
    up_loads = [load(uv_hbm, uv), load(uq_hbm, uq), load(ur_hbm, ur)]
    uk_load = load(uk_hbm, uk)
    table_loads = [load(qbase_hbm.at[sp], qbase), load(qstep_hbm, qstep)]
    ow_load = load(ow_hbm, ow)

    def block(o_, i_, g_, c_):
        return (o_ * 2 + i_) * T + g_ * 2 + c_

    def block_rows(b):
        return pl.ds(pl.multiple_of(b * rows, rows), rows)

    def kv_copy(o_, i_, g_, target, index):
        s = o_ * 2 + i_
        part = kv.at[s * T + g_ * 2 + c]
        return pltpu.make_async_remote_copy(
            src_ref=part,
            dst_ref=part,
            send_sem=kv_send.at[index],
            recv_sem=kv_recv.at[2 * S + s if target is mate else 2 * s + g_],
            device_id=target,
            device_id_type=MESH,
        )

    def kv_wait(o_, i_, g_):
        kv_copy(o_, i_, g_, across, 0).wait_recv()

    def kv_blocks(count, send, receive):
        part = kv.at[pl.ds(0, count)]
        return pltpu.make_async_remote_copy(
            src_ref=part,
            dst_ref=part,
            send_sem=kv_send.at[send],
            recv_sem=kv_recv.at[receive],
            device_id=mate,
            device_id_type=MESH,
        )

    def mate_in(s):
        kv_blocks(2, 0, 2 * S + s).wait_recv()

    wide = 2 * LANES
    mine = block(o, i, g, c)

    side = span // 2

    def phase(body):
        pl.when(sp < S)(body)

    def projected(weight, weight_loads):
        sums = [jnp.zeros((rows, wide), F32) for _ in range(weight.shape[1] // wide)]
        for k in range(chunks):
            weight_loads[k].wait()
            part = tokens[:, k * step : (k + 1) * step]
            for n in range(len(sums)):
                sums[n] += dot(part, weight[k * step : (k + 1) * step, n * wide : (n + 1) * wide])
        return jnp.concatenate(sums, axis=1)

    @phase
    def _():
        tok_load.wait()
        dr_load.wait()
        turned = dot_nt(tokens[...], dr[...])
        latent = projected(dl, dl_loads)
        for copy in key_loads:
            copy.wait()
        lane = lax.broadcasted_iota(jnp.int32, (rows, LANES), 1)
        start_cos, start_sin = kbase[0:1, :], kbase[8:9, :]
        cosine = start_cos * kstep[:rows, :] - start_sin * kstep[rows:, :]
        sine = start_sin * kstep[:rows, :] + start_cos * kstep[rows:, :]
        turned = jnp.concatenate([turned, jnp.zeros((rows, LANES - ROPE), F32)], axis=1)
        low = lane % ROPE < HALF
        swapped = jnp.where(low, -pltpu.roll(turned, LANES - HALF, 1), pltpu.roll(turned, HALF, 1))
        turned = turned * cosine + swapped * sine
        packed = jnp.where(lane[: rows // 2] < ROPE, turned[: rows // 2], pltpu.roll(turned[rows // 2 :], ROPE, 1))
        latent = normed(latent, lg[...]).astype(BF16)
        for k in range(slabs):
            kv[mine, k * rows : (k + 1) * rows, :] = latent[:, k * LANES : (k + 1) * LANES]
        kv[mine, slabs * rows :, :] = packed.astype(BF16)

    pl.semaphore_wait(barrier, O - 1 + 3)

    def up(g_, i_):
        def send(d, allowed):
            @pl.when((o + d < O) & allowed)
            def _():
                kv_copy(o, i_, g_, dev((o + d) % O, i, g, c), O + d - 1).start()

        for d in reversed(range(1, O)):
            send(d, (o > 0) | (d == O - 1))
        for d in range(1, O - 1):
            send(d, (o == 0) & ((d != O - 2) | (O < 4) | (g_ is not g)))

    def relay_column(d):
        @pl.when((d == O - 1) & (O >= 4))
        def _():
            kv_copy(o - d, i, g, dev(O - 2, i, g, c), d).start()

        kv_copy(o - d, i, g, across, d).start()

        @pl.when((i == 0) | (d > 0))
        def _():
            kv_copy(o - d, i, g, beside, d).start()

        kv_copy(o - d, i, g, mate, d).start()

    def column_in(d):
        kv_wait(o - d, i, g)
        relay_column(d)

    def across_in(d):
        kv_wait(o - d, i, 1 - g)
        kv_copy(o - d, i, 1 - g, mate, d).start()

    def beside_in(d):
        kv_wait(o - d, 1 - i, g)
        kv_copy(o - d, 1 - i, g, mate, d).start()

    def corner_in(d):
        kv_wait(o - d, 1 - i, 1 - g)

        @pl.when((i == 1) | (d > 0))
        def _():
            kv_copy(o - d, 1 - i, 1 - g, mate, d).start()

    def each(first, last, body):
        def run(d, carry):
            body(d)
            return carry

        lax.fori_loop(first, last, run, 0)

    up(g, i)
    relay_column(0)

    own_rows = pl.ds(pl.multiple_of(tp * rows, rows), rows)

    @phase
    def _():
        query = projected(dq, dq_loads)
        qg_load.wait()
        ql[own_rows, :] = normed(query, qg[...]).astype(BF16)

    def q_copy(t, target):
        part = ql.at[block_rows(t)]
        return pltpu.make_async_remote_copy(
            src_ref=part,
            dst_ref=part,
            send_sem=q_send.at[0],
            recv_sem=q_recv.at[t],
            device_id=target,
            device_id_type=MESH,
        )

    other = (1 - g) * 2 + c
    q_copy(tp, across).start()
    q_copy(tp, mate).start()

    for copy in up_loads:
        copy.wait()
    uk_load.wait()
    uvt[...] = uv[...].T

    def latents(s):
        return jnp.concatenate(
            [
                jnp.concatenate([kv[s * T + t, k * rows : (k + 1) * rows, :] for k in range(slabs)], axis=1)
                for t in range(T)
            ],
            axis=0,
        )

    def rotaries(s):
        parts = []
        for t in range(T):
            both = kv[s * T + t, slabs * rows :, :].astype(F32)
            parts += [both, pltpu.roll(both, ROPE, 1)]
        return jnp.concatenate(parts, axis=0).astype(BF16)

    def head_parts(s, slot):
        lat = latents(s)

        def key_part(n):
            keys[slot, :, n : n + wide] = dot(lat, uk[:, n : n + wide]).astype(BF16)

        def value_part(n):
            vals[slot, n : n + wide, :] = dot_nt(uvt[n : n + wide, :], lat).astype(BF16)

        def rotary_part():
            rots[slot] = rotaries(s)

        parts = [functools.partial(key_part, n) for n in range(0, heads * NOPE, wide)]
        parts += [functools.partial(value_part, n) for n in range(0, heads * VDIM, wide)]
        return [rotary_part] + parts

    def kv_heads(s, slot):
        for part in head_parts(s, slot):
            part()

    def relay_in(s):
        d, same = o - s // 2, s % 2 == i
        pl.when((d > 0) & same)(lambda: across_in(d))

        @pl.when((d > 0) & jnp.logical_not(same))
        def _():
            beside_in(d)
            corner_in(d)

    across_in(0)

    @pl.when((i == 0) | (o < O - 1))
    def _():
        kv_copy(o, i, 1 - g, beside, 2 * O - 1).start()

    pl.when((o >= 1) & (o == O - 1))(lambda: column_in(1))
    pl.when(i == 1)(lambda: beside_in(0))
    uqt[...] = uq[...].T
    urt[...] = ur[...].T
    mate_in(sp)
    phase(lambda: kv_heads(sp, 0))

    @pl.when((i == 1) | (o < O - 1))
    def _():
        corner_in(0)
        up(1 - g, 1 - i)

    pl.when((o >= 1) & (o < O - 1))(lambda: column_in(1))

    pl.when(o == O - 1)(lambda: each(2, o + 1, column_in))
    q_copy(other, mate).wait_recv()
    q_copy(other, mate).start()

    def seq(j):
        return sp - j - jnp.where(i == 1, 0, 2 * (j % 2) - 1)

    @pl.when(i == 1)
    def _():
        mate_in(seq(1))
        kv_heads(seq(1), 1)

    pl.when((o >= 1) & (o == O - 1))(lambda: across_in(1))
    for copy in table_loads:
        copy.wait()
    q_cos = jnp.concatenate([qbase[:HALF, :]] * (span // LANES), axis=1)
    q_sin = jnp.concatenate([qbase[HALF:, :]] * (span // LANES), axis=1)
    step_cos, step_sin = qstep[:HALF, :], qstep[HALF:, :]
    q_cos, q_sin = q_cos * step_cos - q_sin * step_sin, q_sin * step_cos + q_cos * step_sin
    q_copy(g * 2 + 1 - c, mate).wait_recv()
    q_copy((1 - g) * 2 + 1 - c, mate).wait_recv()

    scale = (NOPE + ROPE) ** (-0.5) * log2e

    @phase
    def _():
        plain = dot_nt(uqt[...], ql[...]) * scale
        turning = dot_nt(urt[...], ql[...]) * scale
        for h in range(heads):
            first = turning[h * ROPE : h * ROPE + HALF, :]
            second = turning[h * ROPE + HALF : (h + 1) * ROPE, :]
            whole = [
                plain[h * NOPE : (h + 1) * NOPE, :],
                first * q_cos - second * q_sin,
                second * q_cos + first * q_sin,
                jnp.zeros((LANES - ROPE, span), F32),
            ]
            whole = jnp.concatenate(whole, axis=0).astype(BF16)
            for n in range(2):
                qt[n, h] = whole[:, n * side : (n + 1) * side]

    def score(slot, h, group):
        key = jnp.concatenate([keys[slot, :, h * NOPE : (h + 1) * NOPE], rots[slot]], axis=1)
        return dot(key, qt[group, h])

    def attend(slot, group, first=False, ahead=None):
        ones = jnp.ones((acc.shape[1] - VDIM, span), BF16)
        parts = [] if ahead is None else head_parts(*ahead)
        if first:
            k_pos = lax.broadcasted_iota(jnp.int32, (span, side), 0)
            q_pos = lax.broadcasted_iota(jnp.int32, (span, side), 1) + group * side
            allowed = k_pos <= q_pos
        later = score(slot, 0, group) if first else scored[...]
        for h in range(heads):
            scores = later
            if h + 1 < heads:
                later = score(slot, h + 1, group)
            for part in parts[h * len(parts) // heads : (h + 1) * len(parts) // heads]:
                part()
            value = jnp.concatenate([vals[slot, h * VDIM : (h + 1) * VDIM, :], ones], axis=0)
            if first:
                scores = jnp.where(allowed, scores, masked_score)
            new = jnp.max(scores, axis=0, keepdims=True)
            if not first:
                old = best[h][:1]
                new = jnp.maximum(old, new)
            weights = jnp.exp2(scores - new).astype(BF16)
            if first:
                acc[h] = dot(value, weights)
            else:
                acc[h] = acc[h] * jnp.exp2(old - new) + dot(value, weights)
            best[h] = jnp.broadcast_to(new, best.shape[1:])
        if ahead is not None:
            scored[...] = score(ahead[1], 0, group)

    def sweep(group, arriving):
        @pl.when(sp >= 1)
        def _():
            def both(j):
                if arriving:
                    pl.when((i == 0) & (j + 2 <= sp))(lambda: relay_in(seq(j + 2)))
                    mate_in(seq(j + 1))
                attend(j % 2, group, ahead=(seq(j + 1), (j + 1) % 2))
                if arriving:
                    pl.when((i == 1) & (j + 3 <= sp))(lambda: relay_in(seq(j + 3)))

            each(1, sp, both)
            attend(sp % 2, group)

        @phase
        def _():
            for h in range(heads):
                whole = acc[h]
                part = (whole[:VDIM] / whole[VDIM : VDIM + 1]).T.astype(BF16)
                att[pl.ds(pl.multiple_of(group * side, side), side), h * VDIM : (h + 1) * VDIM] = part

    phase(lambda: attend(0, 1 - g, first=True))

    @pl.when((o >= 1) & (o < O - 1))
    def _():
        each(2, o + 1, column_in)
        across_in(1)

    @pl.when(o >= 1)
    def _():
        beside_in(1)
        corner_in(1)

    @pl.when(sp >= 1)
    def _():
        @pl.when(i == 0)
        def _():
            mate_in(seq(1))
            kv_heads(seq(1), 1)

        phase(lambda: scored.__setitem__(..., score(1, 0, 1 - g)))

    sweep(1 - g, True)

    ow_load.wait()
    width = ow.shape[1] // pieces
    lag = min(3, pieces)

    def pair_copy(second, j):
        return pltpu.make_async_remote_copy(
            src_ref=pair_out.at[second, j],
            dst_ref=pair_in.at[second, j],
            send_sem=pair_send.at[0],
            recv_sem=pair_recv.at[pieces if second else j],
            device_id=mate,
            device_id_type=MESH,
        )

    def cross_copy(j):
        return pltpu.make_async_remote_copy(
            src_ref=cross_out.at[j],
            dst_ref=cross_in.at[j],
            send_sem=cross_send.at[0],
            recv_sem=cross_recv.at[j],
            device_id=across,
            device_id_type=MESH,
        )

    def project(second, group, j):
        top = att[block_rows(group * 2 + 1 - c), :]
        low_part = att[block_rows(group * 2 + c), :]
        part = dot(jnp.concatenate([top, low_part], axis=0), ow[:, j * width : (j + 1) * width])
        pair_out[second, j] = part[:rows].astype(BF16)
        kept[second, j] = part[rows:]
        pair_copy(second, j).start()

    def cross(j):
        pair_copy(0, j).wait_recv()
        cross_out[j] = (kept[0, j] + pair_in[0, j].astype(F32)).astype(BF16)
        cross_copy(j).start()

    @phase
    def _():
        for j in range(pieces):
            project(0, 1 - g, j)
            if j >= lag:
                cross(j - lag)
        for j in range(pieces - lag, pieces):
            cross(j)

    phase(lambda: kv_heads(sp, 0))
    phase(lambda: attend(0, g, first=True))

    @pl.when(sp >= 1)
    def _():
        kv_heads(seq(1), 1)
        scored[...] = score(1, 0, g)

    sweep(g, False)

    @phase
    def _():
        for j in range(pieces):
            project(1, g, j)

    def all_sent(n, copies):
        pltpu.make_async_remote_copy(
            src_ref=n, dst_ref=n, send_sem=copies.at[0], recv_sem=q_recv.at[0], device_id=mate, device_id_type=MESH
        ).wait_send()

    pl.when(i == 0)(lambda: kv_blocks(4, 0, 0).wait_send())
    pl.when(i == 1)(lambda: kv_blocks(5, 0, 0).wait_send())
    pl.when((i == 0) | (o < O - 1))(lambda: kv_blocks(1, 2 * O - 1, 0).wait_send())

    def some_sent(few, count, index):
        pl.when(few)(lambda: kv_blocks(count - 1, index, 0).wait_send())
        pl.when(jnp.logical_not(few))(lambda: kv_blocks(count, index, 0).wait_send())

    each(1, o + 1, lambda d: some_sent((d < O - 1) | (O < 4), 7, d))
    each(1, O - o, lambda d: some_sent((o == 0) & (d == O - 2) & (O >= 4), 2, O + d - 1))
    all_sent(ql.at[pl.ds(0, 3 * rows)], q_send)
    all_sent(pair_out, pair_send)
    pltpu.make_async_remote_copy(
        src_ref=pair_out.at[1],
        dst_ref=pair_in.at[1],
        send_sem=pair_send.at[0],
        recv_sem=pair_recv.at[pieces],
        device_id=mate,
        device_id_type=MESH,
    ).wait_recv()
    for j in range(pieces):
        cross_copy(j).wait_recv()
        total = kept[1, j] + pair_in[1, j].astype(F32) + cross_in[j].astype(F32)
        out_ref[:, j * width : (j + 1) * width] = total.astype(BF16)
    all_sent(cross_out, cross_send)


def solution(mesh):
    S, T = mesh.shape["sp"], mesh.shape["tp"]
    assert S % 2 == 0 and T == 4

    def local(tokens, dq, dl, dr, qg, lg, uq, ur, uk, uv, ow):
        rows, depth = tokens.shape
        span = rows * T
        heads = uk.shape[1] // NOPE
        width = ow.shape[1]
        rank = dl.shape[1]
        chunks, pieces = 4, 8
        inverse = np.float32(rope_base) ** (-np.arange(0, ROPE, 2, dtype=np.float32) / np.float32(ROPE))
        inverse = inverse.astype(np.float64)
        tiled = np.tile(inverse, LANES // HALF)

        def both(angles, axis):
            return np.concatenate([np.cos(angles), np.sin(angles)], axis=axis)

        key_base = np.repeat((np.arange(S * T) * rows)[:, None, None] * tiled, 8, axis=1)
        key_step = np.arange(rows)[:, None] * tiled
        query_base = np.repeat((np.arange(S) * span)[:, None, None] * inverse[:, None], LANES, axis=2)
        query_step = inverse[:, None] * np.arange(span)
        tables = [
            jnp.asarray(a, F32) for a in (both(key_base, 1), both(key_step, 0), both(query_base, 1), both(query_step, 0))
        ]
        O = S // 2
        hbm = pl.BlockSpec(memory_space=pl.ANY)
        vmem = pl.BlockSpec(memory_space=pltpu.VMEM)
        dma = lambda n: pltpu.SemaphoreType.DMA((n,))
        like = lambda a: pltpu.VMEM(a.shape, a.dtype)
        operands = [tokens, dq, dl, dr.T, qg.reshape(1, -1), lg.reshape(1, -1), uq, ur, uk, uv, ow, *tables]
        operands = [pltpu.with_memory_space_constraint(a, pltpu.HBM) for a in operands]
        block_height = rows * rank // LANES + rows // 2
        return pl.pallas_call(
            functools.partial(kernel, S, T, chunks, pieces),
            out_shape=jax.ShapeDtypeStruct((rows, width), BF16),
            in_specs=[hbm] * len(operands),
            out_specs=vmem,
            scratch_shapes=[
                *[like(a) for a in operands[:11]],
                pltpu.VMEM((16, LANES), F32),
                pltpu.VMEM((2 * rows, LANES), F32),
                pltpu.VMEM((ROPE, LANES), F32),
                pltpu.VMEM((ROPE, span), F32),
                pltpu.VMEM((S * T, block_height, LANES), BF16),
                pltpu.VMEM((span, dq.shape[1]), BF16),
                pltpu.VMEM((2, heads, NOPE + LANES, span // 2), BF16),
                pltpu.VMEM((heads, VDIM + 16, span // 2), F32),
                pltpu.VMEM((heads, 8, span // 2), F32),
                pltpu.VMEM((span, heads * VDIM), BF16),
                pltpu.VMEM((2, pieces, rows, width // pieces), BF16),
                pltpu.VMEM((2, pieces, rows, width // pieces), BF16),
                pltpu.VMEM((2, pieces, rows, width // pieces), F32),
                pltpu.VMEM((pieces, rows, width // pieces), BF16),
                pltpu.VMEM((pieces, rows, width // pieces), BF16),
                pltpu.VMEM(uq.shape[::-1], BF16),
                pltpu.VMEM(ur.shape[::-1], BF16),
                pltpu.VMEM(uv.shape[::-1], BF16),
                pltpu.VMEM((2, span, heads * NOPE), BF16),
                pltpu.VMEM((2, heads * VDIM, span), BF16),
                pltpu.VMEM((2, span, LANES), BF16),
                pltpu.VMEM((span, span // 2), F32),
                dma(2 * chunks + 13),
                dma(2 * O),
                dma(3 * S),
                dma(1),
                dma(T),
                dma(1),
                dma(pieces + 1),
                dma(1),
                dma(pieces),
            ],
            compiler_params=pltpu.CompilerParams(
                collective_id=0, has_side_effects=True, vmem_limit_bytes=46 * 1024 * 1024
            ),
        )(*operands)

    return jax.shard_map(
        local,
        mesh=mesh,
        in_specs=(
            P(("sp", "tp"), None),
            P(),
            P(),
            P(),
            P(),
            P(),
            P(None, "tp"),
            P(None, "tp"),
            P(None, "tp"),
            P(None, "tp"),
            P("tp", None),
        ),
        out_specs=P(("sp", "tp"), None),
        check_vma=False,
    )
```

```python
import functools

import jax
import jax.numpy as jnp
import numpy as np
from jax import lax
from jax.experimental import pallas as pl
from jax.experimental.pallas import tpu as pltpu
from jax.sharding import PartitionSpec as P

NOPE = 128
ROPE = 64
HALF = ROPE // 2
VDIM = 128
LANES = 128

rope_base = 500000.0
norm_eps = 1e-06
masked_score = -1e30
log2e = 1.4426950408889634

MESH = pl.DeviceIdType.MESH
F32 = jnp.float32
BF16 = jnp.bfloat16


def dot(a, b):
    return jnp.dot(a, b, preferred_element_type=F32)


def dot_nt(a, b):
    return lax.dot_general(a, b, (((1,), (1,)), ((), ())), preferred_element_type=F32)


def normed(v, gain):
    return v * lax.rsqrt(jnp.mean(v * v, axis=-1, keepdims=True) + norm_eps) * gain


def kernel(
    S,
    T,
    chunks,
    pieces,
    tokens_hbm,
    dq_hbm,
    dl_hbm,
    dr_hbm,
    qg_hbm,
    lg_hbm,
    uq_hbm,
    ur_hbm,
    uk_hbm,
    uv_hbm,
    ow_hbm,
    kbase_hbm,
    kstep_hbm,
    qbase_hbm,
    qstep_hbm,
    out_ref,
    tokens,
    dq,
    dl,
    dr,
    qg,
    lg,
    uq,
    ur,
    uk,
    uv,
    ow,
    kbase,
    kstep,
    qbase,
    qstep,
    kv,
    ql,
    qt,
    acc,
    best,
    att,
    pair_out,
    pair_in,
    kept,
    cross_out,
    cross_in,
    uqt,
    urt,
    uvt,
    keys0,
    vals0,
    rots0,
    keys1,
    vals1,
    rots1,
    scored,
    load_sem,
    kv_send,
    kv_recv,
    q_send,
    q_recv,
    pair_send,
    pair_recv,
    cross_send,
    cross_recv,
):
    O = S // 2
    keys, vals, rots = (keys0, keys1), (vals0, vals1), (rots0, rots1)
    rows = tokens.shape[0]
    span = rows * T
    depth = tokens.shape[1]
    heads = qt.shape[1]
    rank = dl.shape[1]
    slabs = rank // LANES
    sp = lax.axis_index("sp")
    tp = lax.axis_index("tp")
    o, i = sp // 2, sp % 2
    g, c = tp // 2, tp % 2

    def dev(o_, i_, g_, c_):
        return {"sp": o_ * 2 + i_, "tp": g_ * 2 + c_}

    across = dev(o, i, 1 - g, c)
    beside = dev(o, 1 - i, g, c)
    mate = dev(o, i, g, 1 - c)

    barrier = pltpu.get_barrier_semaphore()
    for d in range(1, O):
        pl.semaphore_signal(barrier, inc=1, device_id=dev((o + d) % O, i, g, c), device_id_type=MESH)
    for target in (across, beside, mate):
        pl.semaphore_signal(barrier, inc=1, device_id=target, device_id_type=MESH)

    step = depth // chunks
    loads = []

    def load(src, dst):
        copy = pltpu.make_async_copy(src, dst, load_sem.at[len(loads)])
        loads.append(copy)
        copy.start()
        return copy

    tok_load = load(tokens_hbm, tokens)
    dr_load = load(dr_hbm, dr)
    dl_loads = [load(dl_hbm.at[pl.ds(k * step, step)], dl.at[pl.ds(k * step, step)]) for k in range(chunks)]
    key_loads = [load(lg_hbm, lg), load(kbase_hbm.at[sp * T + tp], kbase), load(kstep_hbm, kstep)]
    dq_loads = [load(dq_hbm.at[pl.ds(k * step, step)], dq.at[pl.ds(k * step, step)]) for k in range(chunks)]
    qg_load = load(qg_hbm, qg)
    up_loads = [load(uv_hbm, uv), load(uq_hbm, uq), load(ur_hbm, ur)]
    uk_load = load(uk_hbm, uk)
    table_loads = [load(qbase_hbm.at[sp], qbase), load(qstep_hbm, qstep)]
    ow_load = load(ow_hbm, ow)

    def block(o_, i_, g_, c_):
        return (o_ * 2 + i_) * T + g_ * 2 + c_

    def block_rows(b):
        return pl.ds(pl.multiple_of(b * rows, rows), rows)

    def kv_copy(o_, i_, g_, target, index):
        s = o_ * 2 + i_
        part = kv.at[s * T + g_ * 2 + c]
        return pltpu.make_async_remote_copy(
            src_ref=part,
            dst_ref=part,
            send_sem=kv_send.at[index],
            recv_sem=kv_recv.at[2 * S + s if target is mate else 2 * s + g_],
            device_id=target,
            device_id_type=MESH,
        )

    def kv_wait(o_, i_, g_):
        kv_copy(o_, i_, g_, across, 0).wait_recv()

    def kv_blocks(count, send, receive):
        part = kv.at[pl.ds(0, count)]
        return pltpu.make_async_remote_copy(
            src_ref=part,
            dst_ref=part,
            send_sem=kv_send.at[send],
            recv_sem=kv_recv.at[receive],
            device_id=mate,
            device_id_type=MESH,
        )

    def mate_in(s):
        kv_blocks(2, 0, 2 * S + s).wait_recv()

    wide = 2 * LANES
    mine = block(o, i, g, c)

    side = span // 2

    def phase(body):
        pl.when(sp < S)(body)

    def projected(weight, weight_loads):
        sums = [jnp.zeros((rows, wide), F32) for _ in range(weight.shape[1] // wide)]
        for k in range(chunks):
            weight_loads[k].wait()
            part = tokens[:, k * step : (k + 1) * step]
            for n in range(len(sums)):
                sums[n] += dot(part, weight[k * step : (k + 1) * step, n * wide : (n + 1) * wide])
        return jnp.concatenate(sums, axis=1)

    @phase
    def _():
        tok_load.wait()
        dr_load.wait()
        turned = dot_nt(tokens[...], dr[...])
        latent = projected(dl, dl_loads)
        for copy in key_loads:
            copy.wait()
        lane = lax.broadcasted_iota(jnp.int32, (rows, LANES), 1)
        start_cos, start_sin = kbase[0:1, :], kbase[8:9, :]
        cosine = start_cos * kstep[:rows, :] - start_sin * kstep[rows:, :]
        sine = start_sin * kstep[:rows, :] + start_cos * kstep[rows:, :]
        turned = jnp.concatenate([turned, jnp.zeros((rows, LANES - ROPE), F32)], axis=1)
        low = lane % ROPE < HALF
        swapped = jnp.where(low, -pltpu.roll(turned, LANES - HALF, 1), pltpu.roll(turned, HALF, 1))
        turned = turned * cosine + swapped * sine
        packed = jnp.where(lane[: rows // 2] < ROPE, turned[: rows // 2], pltpu.roll(turned[rows // 2 :], ROPE, 1))
        latent = normed(latent, lg[...]).astype(BF16)
        for k in range(slabs):
            kv[mine, k * rows : (k + 1) * rows, :] = latent[:, k * LANES : (k + 1) * LANES]
        kv[mine, slabs * rows :, :] = packed.astype(BF16)

    pl.semaphore_wait(barrier, O - 1 + 3)

    def up(g_, i_):
        def send(d, allowed):
            @pl.when((o + d < O) & allowed)
            def _():
                kv_copy(o, i_, g_, dev((o + d) % O, i, g, c), O + d - 1).start()

        own = g_ is g
        for d in reversed(range(1, O)):
            send(d, ((o > 0) & own) | ((o == 0) & (d == O - 1)))
        for d in range(1, O - 1):
            send(d, (o == 0) & ((d != O - 2) | (O < 4)) if own else o < O)

    def relay_column(d):
        @pl.when((d == O - 1) & (O >= 4))
        def _():
            kv_copy(o - d, i, g, dev(O - 2, i, g, c), d).start()

        kv_copy(o - d, i, g, across, d).start()

        @pl.when((i == 0) | (d > 0))
        def _():
            kv_copy(o - d, i, g, beside, d).start()

        kv_copy(o - d, i, g, mate, d).start()

    def column_in(d):
        kv_wait(o - d, i, g)
        relay_column(d)

    def across_in(d):
        kv_wait(o - d, i, 1 - g)
        kv_copy(o - d, i, 1 - g, mate, d).start()

    def beside_in(d):
        kv_wait(o - d, 1 - i, g)
        kv_copy(o - d, 1 - i, g, mate, d).start()

    def corner_in(d):
        kv_wait(o - d, 1 - i, 1 - g)

        @pl.when((i == 1) | (d > 0))
        def _():
            kv_copy(o - d, 1 - i, 1 - g, mate, d).start()

    def each(first, last, body):
        def run(d, carry):
            body(d)
            return carry

        lax.fori_loop(first, last, run, 0)

    up(g, i)
    relay_column(0)

    own_rows = pl.ds(pl.multiple_of(tp * rows, rows), rows)

    @phase
    def _():
        query = projected(dq, dq_loads)
        qg_load.wait()
        ql[own_rows, :] = normed(query, qg[...]).astype(BF16)

    def q_copy(t, target):
        part = ql.at[block_rows(t)]
        return pltpu.make_async_remote_copy(
            src_ref=part,
            dst_ref=part,
            send_sem=q_send.at[0],
            recv_sem=q_recv.at[t],
            device_id=target,
            device_id_type=MESH,
        )

    other = (1 - g) * 2 + c
    q_copy(tp, across).start()
    q_copy(tp, mate).start()

    for copy in up_loads:
        copy.wait()
    uk_load.wait()
    uvt[...] = uv[...].T

    def latents(s):
        return jnp.concatenate(
            [
                jnp.concatenate([kv[s * T + t, k * rows : (k + 1) * rows, :] for k in range(slabs)], axis=1)
                for t in range(T)
            ],
            axis=0,
        )

    def rotaries(s):
        parts = []
        for t in range(T):
            both = kv[s * T + t, slabs * rows :, :].astype(F32)
            parts += [both, pltpu.roll(both, ROPE, 1)]
        return jnp.concatenate(parts, axis=0).astype(BF16)

    def head_parts(s, slot):
        lat = latents(s)

        def key_part(n):
            keys[slot][:, n : n + wide] = dot(lat, uk[:, n : n + wide]).astype(BF16)

        def value_part(n):
            vals[slot][n : n + wide, :] = dot_nt(uvt[n : n + wide, :], lat).astype(BF16)

        def rotary_part():
            rots[slot][...] = rotaries(s)

        parts = [functools.partial(key_part, n) for n in range(0, heads * NOPE, wide)]
        parts += [functools.partial(value_part, n) for n in range(0, heads * VDIM, wide)]
        return [rotary_part] + parts

    def kv_heads(s, slot):
        for part in head_parts(s, slot):
            part()

    def relay_in(s):
        d, same = o - s // 2, s % 2 == i
        pl.when((d > 0) & same)(lambda: across_in(d))

        @pl.when((d > 0) & jnp.logical_not(same))
        def _():
            beside_in(d)
            corner_in(d)

    across_in(0)

    @pl.when((i == 0) | (o < O - 1))
    def _():
        kv_copy(o, i, 1 - g, beside, 2 * O - 1).start()

    pl.when((o >= 1) & (o == O - 1))(lambda: column_in(1))
    pl.when(i == 1)(lambda: beside_in(0))
    uqt[...] = uq[...].T
    urt[...] = ur[...].T
    mate_in(sp)
    phase(lambda: kv_heads(sp, 0))

    @pl.when((i == 1) | (o < O - 1))
    def _():
        corner_in(0)
        up(1 - g, 1 - i)

    pl.when((o >= 1) & (o < O - 1))(lambda: column_in(1))

    pl.when(o == O - 1)(lambda: each(2, o + 1, column_in))
    q_copy(other, mate).wait_recv()
    q_copy(other, mate).start()

    last = (o == O - 1) & (o >= 3)

    def seq(j):
        m = j + 1 - i
        d = m // 2
        d = jnp.where(last & (d >= 2), jnp.where(d == 2, o, d - 1), d)
        return (o - d) * 2 + jnp.where(m % 2 == 0, i, 1 - i)

    @pl.when(i == 1)
    def _():
        mate_in(seq(1))
        kv_heads(seq(1), 1)

    for copy in table_loads:
        copy.wait()
    q_cos = jnp.concatenate([qbase[:HALF, :]] * (span // LANES), axis=1)
    q_sin = jnp.concatenate([qbase[HALF:, :]] * (span // LANES), axis=1)
    step_cos, step_sin = qstep[:HALF, :], qstep[HALF:, :]
    q_cos, q_sin = q_cos * step_cos - q_sin * step_sin, q_sin * step_cos + q_cos * step_sin
    q_copy(g * 2 + 1 - c, mate).wait_recv()
    q_copy((1 - g) * 2 + 1 - c, mate).wait_recv()

    scale = (NOPE + ROPE) ** (-0.5) * log2e

    @phase
    def _():
        plain = dot_nt(uqt[...], ql[...]) * scale
        turning = dot_nt(urt[...], ql[...]) * scale
        for h in range(heads):
            first = turning[h * ROPE : h * ROPE + HALF, :]
            second = turning[h * ROPE + HALF : (h + 1) * ROPE, :]
            whole = [
                plain[h * NOPE : (h + 1) * NOPE, :],
                first * q_cos - second * q_sin,
                second * q_cos + first * q_sin,
                jnp.zeros((LANES - ROPE, span), F32),
            ]
            whole = jnp.concatenate(whole, axis=0).astype(BF16)
            for n in range(2):
                qt[n, h] = whole[:, n * side : (n + 1) * side]

    def score(slot, h, group):
        key = jnp.concatenate([keys[slot][:, h * NOPE : (h + 1) * NOPE], rots[slot][...]], axis=1)
        return dot(key, qt[group, h])

    def attend(slot, group, first=False, ahead=None):
        ones = jnp.ones((acc.shape[1] - VDIM, span), BF16)
        parts = [[] for _ in range(heads)]
        if ahead is not None:
            todo = head_parts(ahead, 1 - slot)
            for n, part in enumerate(todo):
                parts[max(n - len(todo) + heads, 0)].append(part)
        if first:
            k_pos = lax.broadcasted_iota(jnp.int32, (span, side), 0)
            q_pos = lax.broadcasted_iota(jnp.int32, (span, side), 1) + group * side
            allowed = k_pos <= q_pos

        def weigh(h, scores):
            if first:
                scores = jnp.where(allowed, scores, masked_score)
            new = jnp.max(scores, axis=0, keepdims=True)
            shrink = None
            if not first:
                old = best[h][:1]
                new = jnp.maximum(old, new)
                shrink = jnp.exp2(old - new)
            best[h] = jnp.broadcast_to(new, best.shape[1:])
            return jnp.exp2(scores - new).astype(BF16), shrink

        def gather(h, weights, shrink):
            value = jnp.concatenate([vals[slot][h * VDIM : (h + 1) * VDIM, :], ones], axis=0)
            if first:
                acc[h] = dot(value, weights)
            else:
                acc[h] = acc[h] * shrink + dot(value, weights)

        later = score(slot, 0, group) if first else scored[...]
        weighed = None
        for h in range(heads):
            scores = later
            if h + 1 < heads:
                later = score(slot, h + 1, group)
            elif ahead is not None:
                later = score(1 - slot, 0, group)
            for part in parts[h]:
                part()
            now = weigh(h, scores)
            if weighed is not None:
                gather(h - 1, *weighed)
            weighed = now
        if ahead is not None:
            scored[...] = later
        gather(heads - 1, *weighed)

    def sweep(group, arriving):
        def one(j, slot):
            if arriving:
                early = (i == 0) | ((o < O - 1) & (j >= 2))
                pl.when(early & (j + 2 <= sp))(lambda: relay_in(seq(j + 2)))
                mate_in(seq(j + 1))
            attend(slot, group, ahead=seq(j + 1))
            if arriving:
                pl.when((i == 1) & (o < O - 1) & (j == 1) & (sp >= 3))(lambda: relay_in(seq(3)))
                pl.when((i == 1) & (o == O - 1) & (j + 3 <= sp))(lambda: relay_in(seq(j + 3)))

        @pl.when(sp >= 1)
        def _():
            def two(n):
                one(2 * n + 1, 1)
                one(2 * n + 2, 0)

            each(0, (sp - 1) // 2, two)

            @pl.when(i == 0)
            def _():
                one(sp - 1, 1)
                attend(0, group)

            pl.when(i == 1)(lambda: attend(1, group))

        @phase
        def _():
            for h in range(heads):
                whole = acc[h]
                part = (whole[:VDIM] / whole[VDIM : VDIM + 1]).T.astype(BF16)
                att[pl.ds(pl.multiple_of(group * side, side), side), h * VDIM : (h + 1) * VDIM] = part

    pl.when((o >= 1) & (o == O - 1))(lambda: across_in(1))
    phase(lambda: attend(0, 1 - g, first=True))

    @pl.when((o >= 1) & (o < O - 1))
    def _():
        each(2, o + 1, column_in)
        across_in(1)

    @pl.when((i == 0) & (o >= 1))
    def _():
        mate_in(seq(1))
        kv_heads(seq(1), 1)

    pl.when(sp >= 1)(lambda: scored.__setitem__(..., score(1, 0, 1 - g)))

    @pl.when((o >= 1) & ((i == 0) | (o == O - 1)))
    def _():
        beside_in(1)
        corner_in(1)

    sweep(1 - g, True)

    ow_load.wait()
    width = ow.shape[1] // pieces
    lag = min(3, pieces)

    def pair_copy(second, j):
        return pltpu.make_async_remote_copy(
            src_ref=pair_out.at[second, j],
            dst_ref=pair_in.at[second, j],
            send_sem=pair_send.at[0],
            recv_sem=pair_recv.at[pieces if second else j],
            device_id=mate,
            device_id_type=MESH,
        )

    def cross_copy(j):
        return pltpu.make_async_remote_copy(
            src_ref=cross_out.at[j],
            dst_ref=cross_in.at[j],
            send_sem=cross_send.at[0],
            recv_sem=cross_recv.at[j],
            device_id=across,
            device_id_type=MESH,
        )

    def project(second, group, j):
        top = att[block_rows(group * 2 + 1 - c), :]
        low_part = att[block_rows(group * 2 + c), :]
        part = dot(jnp.concatenate([top, low_part], axis=0), ow[:, j * width : (j + 1) * width])
        pair_out[second, j] = part[:rows].astype(BF16)
        kept[second, j] = part[rows:]
        pair_copy(second, j).start()

    def cross(j):
        pair_copy(0, j).wait_recv()
        cross_out[j] = (kept[0, j] + pair_in[0, j].astype(F32)).astype(BF16)
        cross_copy(j).start()

    @phase
    def _():
        for j in range(pieces):
            project(0, 1 - g, j)
            if j >= lag:
                cross(j - lag)
        for j in range(pieces - lag, pieces):
            cross(j)

    phase(lambda: kv_heads(sp, 0))
    phase(lambda: attend(0, g, first=True))

    @pl.when(sp >= 1)
    def _():
        kv_heads(seq(1), 1)
        scored[...] = score(1, 0, g)

    sweep(g, False)

    @phase
    def _():
        for j in range(pieces):
            project(1, g, j)

    def all_sent(n, copies):
        pltpu.make_async_remote_copy(
            src_ref=n, dst_ref=n, send_sem=copies.at[0], recv_sem=q_recv.at[0], device_id=mate, device_id_type=MESH
        ).wait_send()

    pl.when(i == 0)(lambda: kv_blocks(4, 0, 0).wait_send())
    pl.when(i == 1)(lambda: kv_blocks(5, 0, 0).wait_send())
    pl.when((i == 0) | (o < O - 1))(lambda: kv_blocks(1, 2 * O - 1, 0).wait_send())

    def some_sent(few, count, index):
        pl.when(few)(lambda: kv_blocks(count - 1, index, 0).wait_send())
        pl.when(jnp.logical_not(few))(lambda: kv_blocks(count, index, 0).wait_send())

    each(1, o + 1, lambda d: some_sent((d < O - 1) | (O < 4), 7, d))
    each(1, O - o, lambda d: some_sent((o == 0) & (d == O - 2) & (O >= 4), 2, O + d - 1))
    all_sent(ql.at[pl.ds(0, 3 * rows)], q_send)
    all_sent(pair_out, pair_send)
    pltpu.make_async_remote_copy(
        src_ref=pair_out.at[1],
        dst_ref=pair_in.at[1],
        send_sem=pair_send.at[0],
        recv_sem=pair_recv.at[pieces],
        device_id=mate,
        device_id_type=MESH,
    ).wait_recv()
    for j in range(pieces):
        cross_copy(j).wait_recv()
        total = kept[1, j] + pair_in[1, j].astype(F32) + cross_in[j].astype(F32)
        out_ref[:, j * width : (j + 1) * width] = total.astype(BF16)
    all_sent(cross_out, cross_send)


def solution(mesh):
    S, T = mesh.shape["sp"], mesh.shape["tp"]
    assert S % 2 == 0 and T == 4

    def local(tokens, dq, dl, dr, qg, lg, uq, ur, uk, uv, ow):
        rows, depth = tokens.shape
        span = rows * T
        heads = uk.shape[1] // NOPE
        width = ow.shape[1]
        rank = dl.shape[1]
        chunks, pieces = 4, 8
        inverse = np.float32(rope_base) ** (-np.arange(0, ROPE, 2, dtype=np.float32) / np.float32(ROPE))
        inverse = inverse.astype(np.float64)
        tiled = np.tile(inverse, LANES // HALF)

        def both(angles, axis):
            return np.concatenate([np.cos(angles), np.sin(angles)], axis=axis)

        key_base = np.repeat((np.arange(S * T) * rows)[:, None, None] * tiled, 8, axis=1)
        key_step = np.arange(rows)[:, None] * tiled
        query_base = np.repeat((np.arange(S) * span)[:, None, None] * inverse[:, None], LANES, axis=2)
        query_step = inverse[:, None] * np.arange(span)
        tables = [
            jnp.asarray(a, F32) for a in (both(key_base, 1), both(key_step, 0), both(query_base, 1), both(query_step, 0))
        ]
        O = S // 2
        hbm = pl.BlockSpec(memory_space=pl.ANY)
        vmem = pl.BlockSpec(memory_space=pltpu.VMEM)
        dma = lambda n: pltpu.SemaphoreType.DMA((n,))
        like = lambda a: pltpu.VMEM(a.shape, a.dtype)
        operands = [tokens, dq, dl, dr.T, qg.reshape(1, -1), lg.reshape(1, -1), uq, ur, uk, uv, ow, *tables]
        operands = [pltpu.with_memory_space_constraint(a, pltpu.HBM) for a in operands]
        block_height = rows * rank // LANES + rows // 2
        return pl.pallas_call(
            functools.partial(kernel, S, T, chunks, pieces),
            out_shape=jax.ShapeDtypeStruct((rows, width), BF16),
            in_specs=[hbm] * len(operands),
            out_specs=vmem,
            scratch_shapes=[
                *[like(a) for a in operands[:11]],
                pltpu.VMEM((16, LANES), F32),
                pltpu.VMEM((2 * rows, LANES), F32),
                pltpu.VMEM((ROPE, LANES), F32),
                pltpu.VMEM((ROPE, span), F32),
                pltpu.VMEM((S * T, block_height, LANES), BF16),
                pltpu.VMEM((span, dq.shape[1]), BF16),
                pltpu.VMEM((2, heads, NOPE + LANES, span // 2), BF16),
                pltpu.VMEM((heads, VDIM + 16, span // 2), F32),
                pltpu.VMEM((heads, 8, span // 2), F32),
                pltpu.VMEM((span, heads * VDIM), BF16),
                pltpu.VMEM((2, pieces, rows, width // pieces), BF16),
                pltpu.VMEM((2, pieces, rows, width // pieces), BF16),
                pltpu.VMEM((2, pieces, rows, width // pieces), F32),
                pltpu.VMEM((pieces, rows, width // pieces), BF16),
                pltpu.VMEM((pieces, rows, width // pieces), BF16),
                pltpu.VMEM(uq.shape[::-1], BF16),
                pltpu.VMEM(ur.shape[::-1], BF16),
                pltpu.VMEM(uv.shape[::-1], BF16),
                *[
                    pltpu.VMEM((span, heads * NOPE), BF16),
                    pltpu.VMEM((heads * VDIM, span), BF16),
                    pltpu.VMEM((span, LANES), BF16),
                ]
                * 2,
                pltpu.VMEM((span, span // 2), F32),
                dma(2 * chunks + 13),
                dma(2 * O),
                dma(3 * S),
                dma(1),
                dma(T),
                dma(1),
                dma(pieces + 1),
                dma(1),
                dma(pieces),
            ],
            compiler_params=pltpu.CompilerParams(
                collective_id=0, has_side_effects=True, vmem_limit_bytes=46 * 1024 * 1024
            ),
        )(*operands)

    return jax.shard_map(
        local,
        mesh=mesh,
        in_specs=(
            P(("sp", "tp"), None),
            P(),
            P(),
            P(),
            P(),
            P(),
            P(None, "tp"),
            P(None, "tp"),
            P(None, "tp"),
            P(None, "tp"),
            P("tp", None),
        ),
        out_specs=P(("sp", "tp"), None),
        check_vma=False,
    )
```

```python
import functools

import jax
import jax.numpy as jnp
import numpy as np
from jax import lax
from jax.experimental import pallas as pl
from jax.experimental.pallas import tpu as pltpu
from jax.sharding import PartitionSpec as P

NOPE = 128
ROPE = 64
HALF = ROPE // 2
VDIM = 128
LANES = 128

rope_base = 500000.0
norm_eps = 1e-06
masked_score = -1e30
log2e = 1.4426950408889634

MESH = pl.DeviceIdType.MESH
F32 = jnp.float32
BF16 = jnp.bfloat16


def dot(a, b):
    return jnp.dot(a, b, preferred_element_type=F32)


def dot_nt(a, b):
    return lax.dot_general(a, b, (((1,), (1,)), ((), ())), preferred_element_type=F32)


def normed(v, gain):
    return v * lax.rsqrt(jnp.mean(v * v, axis=-1, keepdims=True) + norm_eps) * gain


def kernel(
    S,
    T,
    chunks,
    pieces,
    tokens_hbm,
    dq_hbm,
    dl_hbm,
    dr_hbm,
    qg_hbm,
    lg_hbm,
    uq_hbm,
    ur_hbm,
    uk_hbm,
    uv_hbm,
    ow_hbm,
    kbase_hbm,
    kstep_hbm,
    qbase_hbm,
    qstep_hbm,
    out_ref,
    tokens,
    dq,
    dl,
    dr,
    qg,
    lg,
    uq,
    ur,
    uk,
    uv,
    ow,
    kbase,
    kstep,
    qbase,
    qstep,
    kv,
    ql,
    qt,
    acc,
    best,
    att,
    pair_out,
    pair_in,
    kept,
    cross_out,
    cross_in,
    uqt,
    urt,
    uvt,
    keys0,
    vals0,
    rots0,
    keys1,
    vals1,
    rots1,
    scored,
    load_sem,
    kv_send,
    kv_recv,
    q_send,
    q_recv,
    pair_send,
    pair_recv,
    cross_send,
    cross_recv,
):
    O = S // 2
    keys, vals, rots = (keys0, keys1), (vals0, vals1), (rots0, rots1)
    rows = tokens.shape[0]
    span = rows * T
    depth = tokens.shape[1]
    heads = qt.shape[1]
    rank = dl.shape[1]
    slabs = rank // LANES
    sp = lax.axis_index("sp")
    tp = lax.axis_index("tp")
    o, i = sp // 2, sp % 2
    g, c = tp // 2, tp % 2

    def dev(o_, i_, g_, c_):
        return {"sp": o_ * 2 + i_, "tp": g_ * 2 + c_}

    across = dev(o, i, 1 - g, c)
    beside = dev(o, 1 - i, g, c)
    mate = dev(o, i, g, 1 - c)

    barrier = pltpu.get_barrier_semaphore()
    for d in range(1, O):
        pl.semaphore_signal(barrier, inc=1, device_id=dev((o + d) % O, i, g, c), device_id_type=MESH)
    for target in (across, beside, mate):
        pl.semaphore_signal(barrier, inc=1, device_id=target, device_id_type=MESH)

    step = depth // chunks
    loads = []

    def load(src, dst):
        copy = pltpu.make_async_copy(src, dst, load_sem.at[len(loads)])
        loads.append(copy)
        copy.start()
        return copy

    tok_load = load(tokens_hbm, tokens)
    dr_load = load(dr_hbm, dr)
    dl_loads = [load(dl_hbm.at[pl.ds(k * step, step)], dl.at[pl.ds(k * step, step)]) for k in range(chunks)]
    key_loads = [load(lg_hbm, lg), load(kbase_hbm.at[sp * T + tp], kbase), load(kstep_hbm, kstep)]
    dq_loads = [load(dq_hbm.at[pl.ds(k * step, step)], dq.at[pl.ds(k * step, step)]) for k in range(chunks)]
    qg_load = load(qg_hbm, qg)
    up_loads = [load(uv_hbm, uv), load(uq_hbm, uq), load(ur_hbm, ur)]
    uk_load = load(uk_hbm, uk)
    table_loads = [load(qbase_hbm.at[sp], qbase), load(qstep_hbm, qstep)]
    ow_load = load(ow_hbm, ow)

    def block(o_, i_, g_, c_):
        return (o_ * 2 + i_) * T + g_ * 2 + c_

    def block_rows(b):
        return pl.ds(pl.multiple_of(b * rows, rows), rows)

    def kv_copy(o_, i_, g_, target, index):
        s = o_ * 2 + i_
        part = kv.at[s * T + g_ * 2 + c]
        return pltpu.make_async_remote_copy(
            src_ref=part,
            dst_ref=part,
            send_sem=kv_send.at[index],
            recv_sem=kv_recv.at[2 * S + s if target is mate else 2 * s + g_],
            device_id=target,
            device_id_type=MESH,
        )

    def kv_wait(o_, i_, g_):
        kv_copy(o_, i_, g_, across, 0).wait_recv()

    def kv_blocks(count, send, receive):
        part = kv.at[pl.ds(0, count)]
        return pltpu.make_async_remote_copy(
            src_ref=part,
            dst_ref=part,
            send_sem=kv_send.at[send],
            recv_sem=kv_recv.at[receive],
            device_id=mate,
            device_id_type=MESH,
        )

    def mate_in(s):
        kv_blocks(2, 0, 2 * S + s).wait_recv()

    wide = 2 * LANES
    mine = block(o, i, g, c)

    side = span // 2

    def phase(body):
        pl.when(sp < S)(body)

    def projected(weight, weight_loads):
        sums = [jnp.zeros((rows, wide), F32) for _ in range(weight.shape[1] // wide)]
        for k in range(chunks):
            weight_loads[k].wait()
            part = tokens[:, k * step : (k + 1) * step]
            for n in range(len(sums)):
                sums[n] += dot(part, weight[k * step : (k + 1) * step, n * wide : (n + 1) * wide])
        return jnp.concatenate(sums, axis=1)

    @phase
    def _():
        tok_load.wait()
        dr_load.wait()
        turned = dot_nt(tokens[...], dr[...])
        latent = projected(dl, dl_loads)
        for copy in key_loads:
            copy.wait()
        lane = lax.broadcasted_iota(jnp.int32, (rows, LANES), 1)
        start_cos, start_sin = kbase[0:1, :], kbase[8:9, :]
        cosine = start_cos * kstep[:rows, :] - start_sin * kstep[rows:, :]
        sine = start_sin * kstep[:rows, :] + start_cos * kstep[rows:, :]
        turned = jnp.concatenate([turned, jnp.zeros((rows, LANES - ROPE), F32)], axis=1)
        low = lane % ROPE < HALF
        swapped = jnp.where(low, -pltpu.roll(turned, LANES - HALF, 1), pltpu.roll(turned, HALF, 1))
        turned = turned * cosine + swapped * sine
        packed = jnp.where(lane[: rows // 2] < ROPE, turned[: rows // 2], pltpu.roll(turned[rows // 2 :], ROPE, 1))
        latent = normed(latent, lg[...]).astype(BF16)
        for k in range(slabs):
            kv[mine, k * rows : (k + 1) * rows, :] = latent[:, k * LANES : (k + 1) * LANES]
        kv[mine, slabs * rows :, :] = packed.astype(BF16)

    pl.semaphore_wait(barrier, O - 1 + 3)

    def up(g_, i_):
        def send(d, allowed):
            @pl.when((o + d < O) & allowed)
            def _():
                kv_copy(o, i_, g_, dev((o + d) % O, i, g, c), O + d - 1).start()

        own = g_ is g
        for d in reversed(range(1, O)):
            send(d, ((o > 0) & own) | ((o == 0) & (d == O - 1)))
        for d in range(1, O - 1):
            send(d, (o == 0) & ((d != O - 2) | (O < 4)) if own else o < O)

    def relay_column(d):
        @pl.when((d == O - 1) & (O >= 4))
        def _():
            kv_copy(o - d, i, g, dev(O - 2, i, g, c), d).start()

        @pl.when(d != 1)
        def _():
            kv_copy(o - d, i, g, across, d).start()

        @pl.when((i == 0) | (d > 0))
        def _():
            kv_copy(o - d, i, g, beside, d).start()

        kv_copy(o - d, i, g, mate, d).start()

    def column_in(d):
        kv_wait(o - d, i, g)
        relay_column(d)

    def across_in(d):
        kv_wait(o - d, i, 1 - g)
        kv_copy(o - d, i, 1 - g, mate, d).start()

    def beside_in(d):
        kv_wait(o - d, 1 - i, g)
        kv_copy(o - d, 1 - i, g, mate, d).start()

    def corner_in(d):
        kv_wait(o - d, 1 - i, 1 - g)

        @pl.when((i == 1) | (d > 0))
        def _():
            kv_copy(o - d, 1 - i, 1 - g, mate, d).start()

    def each(first, last, body):
        def run(d, carry):
            body(d)
            return carry

        lax.fori_loop(first, last, run, 0)

    up(g, i)
    relay_column(0)

    own_rows = pl.ds(pl.multiple_of(tp * rows, rows), rows)

    @phase
    def _():
        query = projected(dq, dq_loads)
        qg_load.wait()
        ql[own_rows, :] = normed(query, qg[...]).astype(BF16)

    def q_copy(t, target):
        part = ql.at[block_rows(t)]
        return pltpu.make_async_remote_copy(
            src_ref=part,
            dst_ref=part,
            send_sem=q_send.at[0],
            recv_sem=q_recv.at[t],
            device_id=target,
            device_id_type=MESH,
        )

    other = (1 - g) * 2 + c
    q_copy(tp, across).start()
    q_copy(tp, mate).start()

    for copy in up_loads:
        copy.wait()
    uk_load.wait()
    uvt[...] = uv[...].T

    def latents(s):
        return jnp.concatenate(
            [
                jnp.concatenate([kv[s * T + t, k * rows : (k + 1) * rows, :] for k in range(slabs)], axis=1)
                for t in range(T)
            ],
            axis=0,
        )

    def rotaries(s):
        parts = []
        for t in range(T):
            both = kv[s * T + t, slabs * rows :, :].astype(F32)
            parts += [both, pltpu.roll(both, ROPE, 1)]
        return jnp.concatenate(parts, axis=0).astype(BF16)

    def head_parts(s, slot):
        lat = latents(s)

        def key_part(n):
            keys[slot][:, n : n + wide] = dot(lat, uk[:, n : n + wide]).astype(BF16)

        def value_part(n):
            vals[slot][n : n + wide, :] = dot_nt(uvt[n : n + wide, :], lat).astype(BF16)

        def rotary_part():
            rots[slot][...] = rotaries(s)

        parts = [functools.partial(key_part, n) for n in range(0, heads * NOPE, wide)]
        parts += [functools.partial(value_part, n) for n in range(0, heads * VDIM, wide)]
        return [rotary_part] + parts

    def kv_heads(s, slot):
        for part in head_parts(s, slot):
            part()

    def relay_in(s):
        d, same = o - s // 2, s % 2 == i
        pl.when((d > 0) & same)(lambda: across_in(d))

        @pl.when((d > 0) & jnp.logical_not(same))
        def _():
            beside_in(d)
            corner_in(d)

    across_in(0)

    @pl.when((i == 0) | (o < O - 1))
    def _():
        kv_copy(o, i, 1 - g, beside, 2 * O - 1).start()

    @pl.when(o < O - 1)
    def _():
        kv_copy(o, i, 1 - g, dev((o + 1) % O, i, g, c), O).start()

    def own_heads():
        mate_in(sp)
        kv_heads(sp, 0)

    pl.when(o == O - 1)(lambda: each(1, o + 1, column_in))
    pl.when(i == 1)(lambda: beside_in(0))
    uqt[...] = uq[...].T
    urt[...] = ur[...].T
    pl.when(o < O - 1)(own_heads)

    @pl.when((i == 1) | (o < O - 1))
    def _():
        corner_in(0)
        up(1 - g, 1 - i)

    pl.when((o >= 1) & (o < O - 1))(lambda: column_in(1))
    q_copy(other, mate).wait_recv()
    q_copy(other, mate).start()
    pl.when(o == O - 1)(own_heads)

    last = (o == O - 1) & (o >= 3)

    def seq(j):
        m = j + 1 - i
        d = m // 2
        d = jnp.where(last & (d >= 2), jnp.where(d == 2, o, d - 1), d)
        return (o - d) * 2 + jnp.where(m % 2 == 0, i, 1 - i)

    @pl.when(i == 1)
    def _():
        mate_in(seq(1))
        kv_heads(seq(1), 1)

    for copy in table_loads:
        copy.wait()
    q_cos = jnp.concatenate([qbase[:HALF, :]] * (span // LANES), axis=1)
    q_sin = jnp.concatenate([qbase[HALF:, :]] * (span // LANES), axis=1)
    step_cos, step_sin = qstep[:HALF, :], qstep[HALF:, :]
    q_cos, q_sin = q_cos * step_cos - q_sin * step_sin, q_sin * step_cos + q_cos * step_sin
    q_copy(g * 2 + 1 - c, mate).wait_recv()
    q_copy((1 - g) * 2 + 1 - c, mate).wait_recv()

    scale = (NOPE + ROPE) ** (-0.5) * log2e

    @phase
    def _():
        plain = dot_nt(uqt[...], ql[...]) * scale
        turning = dot_nt(urt[...], ql[...]) * scale
        for h in range(heads):
            first = turning[h * ROPE : h * ROPE + HALF, :]
            second = turning[h * ROPE + HALF : (h + 1) * ROPE, :]
            whole = [
                plain[h * NOPE : (h + 1) * NOPE, :],
                first * q_cos - second * q_sin,
                second * q_cos + first * q_sin,
                jnp.zeros((LANES - ROPE, span), F32),
            ]
            whole = jnp.concatenate(whole, axis=0).astype(BF16)
            for n in range(2):
                qt[n, h] = whole[:, n * side : (n + 1) * side]

    def score(slot, h, group):
        key = jnp.concatenate([keys[slot][:, h * NOPE : (h + 1) * NOPE], rots[slot][...]], axis=1)
        return dot(key, qt[group, h])

    def attend(slot, group, first=False, ahead=None):
        ones = jnp.ones((acc.shape[1] - VDIM, span), BF16)
        parts = [[] for _ in range(heads)]
        if ahead is not None:
            todo = head_parts(ahead, 1 - slot)
            for n, part in enumerate(todo):
                parts[max(n - len(todo) + heads, 0)].append(part)
        if first:
            k_pos = lax.broadcasted_iota(jnp.int32, (span, side), 0)
            q_pos = lax.broadcasted_iota(jnp.int32, (span, side), 1) + group * side
            allowed = k_pos <= q_pos

        def weigh(h, scores):
            if first:
                scores = jnp.where(allowed, scores, masked_score)
            new = jnp.max(scores, axis=0, keepdims=True)
            shrink = None
            if not first:
                old = best[h][:1]
                new = jnp.maximum(old, new)
                shrink = jnp.exp2(old - new)
            best[h] = jnp.broadcast_to(new, best.shape[1:])
            return jnp.exp2(scores - new).astype(BF16), shrink

        def gather(h, weights, shrink):
            value = jnp.concatenate([vals[slot][h * VDIM : (h + 1) * VDIM, :], ones], axis=0)
            if first:
                acc[h] = dot(value, weights)
            else:
                acc[h] = acc[h] * shrink + dot(value, weights)

        later = score(slot, 0, group) if first else scored[...]
        weighed = None
        for h in range(heads):
            scores = later
            if h + 1 < heads:
                later = score(slot, h + 1, group)
            elif ahead is not None:
                later = score(1 - slot, 0, group)
            for part in parts[h]:
                part()
            now = weigh(h, scores)
            if weighed is not None:
                gather(h - 1, *weighed)
            weighed = now
        if ahead is not None:
            scored[...] = later
        gather(heads - 1, *weighed)

    def sweep(group, arriving):
        def one(j, slot):
            if arriving:
                early = (i == 0) | ((o < O - 1) & (j >= 2))
                pl.when(early & (j + 2 <= sp))(lambda: relay_in(seq(j + 2)))
                mate_in(seq(j + 1))
            attend(slot, group, ahead=seq(j + 1))
            if arriving:
                pl.when((i == 1) & (o < O - 1) & (j == 1) & (sp >= 3))(lambda: relay_in(seq(3)))
                pl.when((i == 1) & (o == O - 1) & (j + 3 <= sp))(lambda: relay_in(seq(j + 3)))

        @pl.when(sp >= 1)
        def _():
            def two(n):
                one(2 * n + 1, 1)
                one(2 * n + 2, 0)

            each(0, (sp - 1) // 2, two)

            @pl.when(i == 0)
            def _():
                one(sp - 1, 1)
                attend(0, group)

            pl.when(i == 1)(lambda: attend(1, group))

        @phase
        def _():
            for h in range(heads):
                whole = acc[h]
                part = (whole[:VDIM] / whole[VDIM : VDIM + 1]).T.astype(BF16)
                att[pl.ds(pl.multiple_of(group * side, side), side), h * VDIM : (h + 1) * VDIM] = part

    pl.when((o >= 1) & (o == O - 1))(lambda: across_in(1))
    phase(lambda: attend(0, 1 - g, first=True))

    @pl.when((o >= 1) & (o < O - 1))
    def _():
        each(2, o + 1, column_in)
        across_in(1)

    @pl.when((i == 0) & (o >= 1))
    def _():
        mate_in(seq(1))
        kv_heads(seq(1), 1)

    pl.when(sp >= 1)(lambda: scored.__setitem__(..., score(1, 0, 1 - g)))

    @pl.when((o >= 1) & ((i == 0) | (o == O - 1)))
    def _():
        beside_in(1)
        corner_in(1)

    sweep(1 - g, True)

    ow_load.wait()
    width = ow.shape[1] // pieces
    lag = min(3, pieces)

    def pair_copy(second, j):
        return pltpu.make_async_remote_copy(
            src_ref=pair_out.at[second, j],
            dst_ref=pair_in.at[second, j],
            send_sem=pair_send.at[0],
            recv_sem=pair_recv.at[pieces if second else j],
            device_id=mate,
            device_id_type=MESH,
        )

    def cross_copy(j):
        return pltpu.make_async_remote_copy(
            src_ref=cross_out.at[j],
            dst_ref=cross_in.at[j],
            send_sem=cross_send.at[0],
            recv_sem=cross_recv.at[j],
            device_id=across,
            device_id_type=MESH,
        )

    def project(second, group, j):
        top = att[block_rows(group * 2 + 1 - c), :]
        low_part = att[block_rows(group * 2 + c), :]
        part = dot(jnp.concatenate([top, low_part], axis=0), ow[:, j * width : (j + 1) * width])
        pair_out[second, j] = part[:rows].astype(BF16)
        kept[second, j] = part[rows:]
        pair_copy(second, j).start()

    def cross(j):
        pair_copy(0, j).wait_recv()
        cross_out[j] = (kept[0, j] + pair_in[0, j].astype(F32)).astype(BF16)
        cross_copy(j).start()

    @phase
    def _():
        for j in range(pieces):
            project(0, 1 - g, j)
            if j >= lag:
                cross(j - lag)
        for j in range(pieces - lag, pieces):
            cross(j)

    phase(lambda: kv_heads(sp, 0))
    phase(lambda: attend(0, g, first=True))

    @pl.when(sp >= 1)
    def _():
        kv_heads(seq(1), 1)
        scored[...] = score(1, 0, g)

    sweep(g, False)

    @phase
    def _():
        for j in range(pieces):
            project(1, g, j)

    def all_sent(n, copies):
        pltpu.make_async_remote_copy(
            src_ref=n, dst_ref=n, send_sem=copies.at[0], recv_sem=q_recv.at[0], device_id=mate, device_id_type=MESH
        ).wait_send()

    pl.when(i == 0)(lambda: kv_blocks(4, 0, 0).wait_send())
    pl.when(i == 1)(lambda: kv_blocks(5, 0, 0).wait_send())
    pl.when((i == 0) | (o < O - 1))(lambda: kv_blocks(1, 2 * O - 1, 0).wait_send())

    def counted(index, count, counts):
        for n in counts:
            pl.when(count == n)(lambda n=n: kv_blocks(n, index, 0).wait_send())

    def relays_sent(d):
        counted(d, 6 - jnp.where(d == 1, 1, 0) + jnp.where((d == O - 1) & (O >= 4), 1, 0), (5, 6, 7))

    def ups_sent(d):
        skipped = (o == 0) & (d == O - 2) & (O >= 4)
        counted(O + d - 1, 2 + jnp.where(d == 1, 1, 0) - jnp.where(skipped, 1, 0), (1, 2, 3))

    each(1, o + 1, relays_sent)
    each(1, O - o, ups_sent)
    all_sent(ql.at[pl.ds(0, 3 * rows)], q_send)
    all_sent(pair_out, pair_send)
    pltpu.make_async_remote_copy(
        src_ref=pair_out.at[1],
        dst_ref=pair_in.at[1],
        send_sem=pair_send.at[0],
        recv_sem=pair_recv.at[pieces],
        device_id=mate,
        device_id_type=MESH,
    ).wait_recv()
    for j in range(pieces):
        cross_copy(j).wait_recv()
        total = kept[1, j] + pair_in[1, j].astype(F32) + cross_in[j].astype(F32)
        out_ref[:, j * width : (j + 1) * width] = total.astype(BF16)
    all_sent(cross_out, cross_send)


def solution(mesh):
    S, T = mesh.shape["sp"], mesh.shape["tp"]
    assert S % 2 == 0 and T == 4

    def local(tokens, dq, dl, dr, qg, lg, uq, ur, uk, uv, ow):
        rows, depth = tokens.shape
        span = rows * T
        heads = uk.shape[1] // NOPE
        width = ow.shape[1]
        rank = dl.shape[1]
        chunks, pieces = 4, 8
        inverse = np.float32(rope_base) ** (-np.arange(0, ROPE, 2, dtype=np.float32) / np.float32(ROPE))
        inverse = inverse.astype(np.float64)
        tiled = np.tile(inverse, LANES // HALF)

        def both(angles, axis):
            return np.concatenate([np.cos(angles), np.sin(angles)], axis=axis)

        key_base = np.repeat((np.arange(S * T) * rows)[:, None, None] * tiled, 8, axis=1)
        key_step = np.arange(rows)[:, None] * tiled
        query_base = np.repeat((np.arange(S) * span)[:, None, None] * inverse[:, None], LANES, axis=2)
        query_step = inverse[:, None] * np.arange(span)
        tables = [
            jnp.asarray(a, F32) for a in (both(key_base, 1), both(key_step, 0), both(query_base, 1), both(query_step, 0))
        ]
        O = S // 2
        hbm = pl.BlockSpec(memory_space=pl.ANY)
        vmem = pl.BlockSpec(memory_space=pltpu.VMEM)
        dma = lambda n: pltpu.SemaphoreType.DMA((n,))
        like = lambda a: pltpu.VMEM(a.shape, a.dtype)
        operands = [tokens, dq, dl, dr.T, qg.reshape(1, -1), lg.reshape(1, -1), uq, ur, uk, uv, ow, *tables]
        operands = [pltpu.with_memory_space_constraint(a, pltpu.HBM) for a in operands]
        block_height = rows * rank // LANES + rows // 2
        return pl.pallas_call(
            functools.partial(kernel, S, T, chunks, pieces),
            out_shape=jax.ShapeDtypeStruct((rows, width), BF16),
            in_specs=[hbm] * len(operands),
            out_specs=vmem,
            scratch_shapes=[
                *[like(a) for a in operands[:11]],
                pltpu.VMEM((16, LANES), F32),
                pltpu.VMEM((2 * rows, LANES), F32),
                pltpu.VMEM((ROPE, LANES), F32),
                pltpu.VMEM((ROPE, span), F32),
                pltpu.VMEM((S * T, block_height, LANES), BF16),
                pltpu.VMEM((span, dq.shape[1]), BF16),
                pltpu.VMEM((2, heads, NOPE + LANES, span // 2), BF16),
                pltpu.VMEM((heads, VDIM + 16, span // 2), F32),
                pltpu.VMEM((heads, 8, span // 2), F32),
                pltpu.VMEM((span, heads * VDIM), BF16),
                pltpu.VMEM((2, pieces, rows, width // pieces), BF16),
                pltpu.VMEM((2, pieces, rows, width // pieces), BF16),
                pltpu.VMEM((2, pieces, rows, width // pieces), F32),
                pltpu.VMEM((pieces, rows, width // pieces), BF16),
                pltpu.VMEM((pieces, rows, width // pieces), BF16),
                pltpu.VMEM(uq.shape[::-1], BF16),
                pltpu.VMEM(ur.shape[::-1], BF16),
                pltpu.VMEM(uv.shape[::-1], BF16),
                *[
                    pltpu.VMEM((span, heads * NOPE), BF16),
                    pltpu.VMEM((heads * VDIM, span), BF16),
                    pltpu.VMEM((span, LANES), BF16),
                ]
                * 2,
                pltpu.VMEM((span, span // 2), F32),
                dma(2 * chunks + 13),
                dma(2 * O),
                dma(3 * S),
                dma(1),
                dma(T),
                dma(1),
                dma(pieces + 1),
                dma(1),
                dma(pieces),
            ],
            compiler_params=pltpu.CompilerParams(
                collective_id=0, has_side_effects=True, vmem_limit_bytes=46 * 1024 * 1024
            ),
        )(*operands)

    return jax.shard_map(
        local,
        mesh=mesh,
        in_specs=(
            P(("sp", "tp"), None),
            P(),
            P(),
            P(),
            P(),
            P(),
            P(None, "tp"),
            P(None, "tp"),
            P(None, "tp"),
            P(None, "tp"),
            P("tp", None),
        ),
        out_specs=P(("sp", "tp"), None),
        check_vma=False,
    )
```

```python
import functools

import jax
import jax.numpy as jnp
import numpy as np
from jax import lax
from jax.experimental import pallas as pl
from jax.experimental.pallas import tpu as pltpu
from jax.sharding import PartitionSpec as P

NOPE = 128
ROPE = 64
HALF = ROPE // 2
VDIM = 128
LANES = 128

rope_base = 500000.0
norm_eps = 1e-06
masked_score = -1e30
log2e = 1.4426950408889634

MESH = pl.DeviceIdType.MESH
F32 = jnp.float32
BF16 = jnp.bfloat16


def dot(a, b):
    return jnp.dot(a, b, preferred_element_type=F32)


def dot_nt(a, b):
    return lax.dot_general(a, b, (((1,), (1,)), ((), ())), preferred_element_type=F32)


def normed(v, gain):
    return v * lax.rsqrt(jnp.mean(v * v, axis=-1, keepdims=True) + norm_eps) * gain


def kernel(
    S,
    T,
    chunks,
    pieces,
    tokens_hbm,
    dq_hbm,
    dl_hbm,
    dr_hbm,
    qg_hbm,
    lg_hbm,
    uq_hbm,
    ur_hbm,
    uk_hbm,
    uv_hbm,
    ow_hbm,
    kbase_hbm,
    kstep_hbm,
    qbase_hbm,
    qstep_hbm,
    out_ref,
    tokens,
    dq,
    dl,
    dr,
    qg,
    lg,
    uq,
    ur,
    uk,
    uv,
    ow,
    kbase,
    kstep,
    qbase,
    qstep,
    kv,
    ql,
    qt,
    acc,
    best,
    att,
    pair_out,
    pair_in,
    kept,
    cross_out,
    cross_in,
    uqt,
    urt,
    uvt,
    keys0,
    vals0,
    rots0,
    keys1,
    vals1,
    rots1,
    scored,
    load_sem,
    kv_send,
    kv_recv,
    q_send,
    q_recv,
    pair_send,
    pair_recv,
    cross_send,
    cross_recv,
):
    O = S // 2
    keys, vals, rots = (keys0, keys1), (vals0, vals1), (rots0, rots1)
    rows = tokens.shape[0]
    span = rows * T
    depth = tokens.shape[1]
    heads = qt.shape[1]
    rank = dl.shape[1]
    slabs = rank // LANES
    sp = lax.axis_index("sp")
    tp = lax.axis_index("tp")
    o, i = sp // 2, sp % 2
    g, c = tp // 2, tp % 2

    def dev(o_, i_, g_, c_):
        return {"sp": o_ * 2 + i_, "tp": g_ * 2 + c_}

    across = dev(o, i, 1 - g, c)
    beside = dev(o, 1 - i, g, c)
    mate = dev(o, i, g, 1 - c)

    barrier = pltpu.get_barrier_semaphore()
    for d in range(1, O):
        pl.semaphore_signal(barrier, inc=1, device_id=dev((o + d) % O, i, g, c), device_id_type=MESH)
    for target in (across, beside, mate):
        pl.semaphore_signal(barrier, inc=1, device_id=target, device_id_type=MESH)

    step = depth // chunks
    loads = []

    def load(src, dst):
        copy = pltpu.make_async_copy(src, dst, load_sem.at[len(loads)])
        loads.append(copy)
        copy.start()
        return copy

    tok_load = load(tokens_hbm, tokens)
    dr_load = load(dr_hbm, dr)
    dl_loads = [load(dl_hbm.at[pl.ds(k * step, step)], dl.at[pl.ds(k * step, step)]) for k in range(chunks)]
    key_loads = [load(lg_hbm, lg), load(kbase_hbm.at[sp * T + tp], kbase), load(kstep_hbm, kstep)]
    dq_loads = [load(dq_hbm.at[pl.ds(k * step, step)], dq.at[pl.ds(k * step, step)]) for k in range(chunks)]
    qg_load = load(qg_hbm, qg)
    up_loads = [load(uv_hbm, uv), load(uq_hbm, uq), load(ur_hbm, ur)]
    uk_load = load(uk_hbm, uk)
    table_loads = [load(qbase_hbm.at[sp], qbase), load(qstep_hbm, qstep)]
    ow_load = load(ow_hbm, ow)

    def block(o_, i_, g_, c_):
        return (o_ * 2 + i_) * T + g_ * 2 + c_

    def block_rows(b):
        return pl.ds(pl.multiple_of(b * rows, rows), rows)

    def kv_copy(o_, i_, g_, target, index):
        s = o_ * 2 + i_
        part = kv.at[s * T + g_ * 2 + c]
        return pltpu.make_async_remote_copy(
            src_ref=part,
            dst_ref=part,
            send_sem=kv_send.at[index],
            recv_sem=kv_recv.at[2 * S + s if target is mate else 2 * s + g_],
            device_id=target,
            device_id_type=MESH,
        )

    def kv_wait(o_, i_, g_):
        kv_copy(o_, i_, g_, across, 0).wait_recv()

    def kv_blocks(count, send, receive):
        part = kv.at[pl.ds(0, count)]
        return pltpu.make_async_remote_copy(
            src_ref=part,
            dst_ref=part,
            send_sem=kv_send.at[send],
            recv_sem=kv_recv.at[receive],
            device_id=mate,
            device_id_type=MESH,
        )

    def mate_in(s):
        kv_blocks(2, 0, 2 * S + s).wait_recv()

    wide = 2 * LANES
    mine = block(o, i, g, c)

    side = span // 2

    def phase(body):
        pl.when(sp < S)(body)

    def projected(weight, weight_loads):
        sums = [jnp.zeros((rows, wide), F32) for _ in range(weight.shape[1] // wide)]
        for k in range(chunks):
            weight_loads[k].wait()
            part = tokens[:, k * step : (k + 1) * step]
            for n in range(len(sums)):
                sums[n] += dot(part, weight[k * step : (k + 1) * step, n * wide : (n + 1) * wide])
        return jnp.concatenate(sums, axis=1)

    @phase
    def _():
        tok_load.wait()
        dr_load.wait()
        turned = dot_nt(tokens[...], dr[...])
        latent = projected(dl, dl_loads)
        for copy in key_loads:
            copy.wait()
        lane = lax.broadcasted_iota(jnp.int32, (rows, LANES), 1)
        start_cos, start_sin = kbase[0:1, :], kbase[8:9, :]
        cosine = start_cos * kstep[:rows, :] - start_sin * kstep[rows:, :]
        sine = start_sin * kstep[:rows, :] + start_cos * kstep[rows:, :]
        turned = jnp.concatenate([turned, jnp.zeros((rows, LANES - ROPE), F32)], axis=1)
        low = lane % ROPE < HALF
        swapped = jnp.where(low, -pltpu.roll(turned, LANES - HALF, 1), pltpu.roll(turned, HALF, 1))
        turned = turned * cosine + swapped * sine
        packed = jnp.where(lane[: rows // 2] < ROPE, turned[: rows // 2], pltpu.roll(turned[rows // 2 :], ROPE, 1))
        latent = normed(latent, lg[...]).astype(BF16)
        for k in range(slabs):
            kv[mine, k * rows : (k + 1) * rows, :] = latent[:, k * LANES : (k + 1) * LANES]
        kv[mine, slabs * rows :, :] = packed.astype(BF16)

    pl.semaphore_wait(barrier, O - 1 + 3)

    def up(g_, i_):
        def send(d, allowed):
            @pl.when((o + d < O) & allowed)
            def _():
                kv_copy(o, i_, g_, dev((o + d) % O, i, g, c), O + d - 1).start()

        own = g_ is g
        for d in reversed(range(1, O)):
            send(d, ((o > 0) & own) | ((o == 0) & (d == O - 1)))
        for d in range(1, O - 1):
            send(d, (o == 0) & ((d != O - 2) | (O < 4)) if own else o < O)

    def relay_column(d):
        @pl.when((d == O - 1) & (O >= 4))
        def _():
            kv_copy(o - d, i, g, dev(O - 2, i, g, c), d).start()

        @pl.when(d != 1)
        def _():
            kv_copy(o - d, i, g, across, d).start()

        @pl.when((i == 0) | (d > 0))
        def _():
            kv_copy(o - d, i, g, beside, d).start()

        kv_copy(o - d, i, g, mate, d).start()

    def column_in(d):
        kv_wait(o - d, i, g)
        relay_column(d)

    def across_in(d):
        kv_wait(o - d, i, 1 - g)
        kv_copy(o - d, i, 1 - g, mate, d).start()

    def beside_in(d):
        kv_wait(o - d, 1 - i, g)
        kv_copy(o - d, 1 - i, g, mate, d).start()

    def corner_in(d):
        kv_wait(o - d, 1 - i, 1 - g)

        @pl.when((i == 1) | (d > 0))
        def _():
            kv_copy(o - d, 1 - i, 1 - g, mate, d).start()

    def each(first, last, body):
        def run(d, carry):
            body(d)
            return carry

        lax.fori_loop(first, last, run, 0)

    up(g, i)
    relay_column(0)

    own_rows = pl.ds(pl.multiple_of(tp * rows, rows), rows)

    @phase
    def _():
        query = projected(dq, dq_loads)
        qg_load.wait()
        ql[own_rows, :] = normed(query, qg[...]).astype(BF16)

    def q_copy(t, target):
        part = ql.at[block_rows(t)]
        return pltpu.make_async_remote_copy(
            src_ref=part,
            dst_ref=part,
            send_sem=q_send.at[0],
            recv_sem=q_recv.at[t],
            device_id=target,
            device_id_type=MESH,
        )

    other = (1 - g) * 2 + c
    q_copy(tp, across).start()
    q_copy(tp, mate).start()

    for copy in up_loads:
        copy.wait()
    uk_load.wait()
    uvt[...] = uv[...].T

    def latents(s):
        return jnp.concatenate(
            [
                jnp.concatenate([kv[s * T + t, k * rows : (k + 1) * rows, :] for k in range(slabs)], axis=1)
                for t in range(T)
            ],
            axis=0,
        )

    def rotaries(s):
        parts = []
        for t in range(T):
            both = kv[s * T + t, slabs * rows :, :].astype(F32)
            parts += [both, pltpu.roll(both, ROPE, 1)]
        return jnp.concatenate(parts, axis=0).astype(BF16)

    def head_parts(s, slot):
        lat = latents(s)

        def key_part(n):
            keys[slot][:, n : n + wide] = dot(lat, uk[:, n : n + wide]).astype(BF16)

        def value_part(n):
            vals[slot][n : n + wide, :] = dot_nt(uvt[n : n + wide, :], lat).astype(BF16)

        def rotary_part():
            rots[slot][...] = rotaries(s)

        parts = [functools.partial(key_part, n) for n in range(0, heads * NOPE, wide)]
        parts += [functools.partial(value_part, n) for n in range(0, heads * VDIM, wide)]
        return [rotary_part] + parts

    def kv_heads(s, slot):
        for part in head_parts(s, slot):
            part()

    def relay_in(s):
        d, same = o - s // 2, s % 2 == i
        pl.when((d > 0) & same)(lambda: across_in(d))

        @pl.when((d > 0) & jnp.logical_not(same))
        def _():
            beside_in(d)
            corner_in(d)

    across_in(0)

    @pl.when((i == 0) | (o < O - 1))
    def _():
        kv_copy(o, i, 1 - g, beside, 2 * O - 1).start()

    @pl.when(o < O - 1)
    def _():
        kv_copy(o, i, 1 - g, dev((o + 1) % O, i, g, c), O).start()

    def own_heads():
        mate_in(sp)
        kv_heads(sp, 0)

    pl.when(o == O - 1)(lambda: each(1, o + 1, column_in))
    pl.when(i == 1)(lambda: beside_in(0))
    uqt[...] = uq[...].T
    urt[...] = ur[...].T
    pl.when(o < O - 1)(own_heads)

    @pl.when((i == 1) | (o < O - 1))
    def _():
        corner_in(0)
        up(1 - g, 1 - i)

    pl.when((o >= 1) & (o < O - 1))(lambda: column_in(1))
    q_copy(other, mate).wait_recv()
    q_copy(other, mate).start()
    pl.when(o == O - 1)(own_heads)

    last = (o == O - 1) & (o >= 3)

    def seq(j):
        m = j + 1 - i
        d = m // 2
        d = jnp.where(last & (d >= 2), jnp.where(d == 2, o, d - 1), d)
        return (o - d) * 2 + jnp.where(m % 2 == 0, i, 1 - i)

    @pl.when(i == 1)
    def _():
        mate_in(seq(1))
        kv_heads(seq(1), 1)

    for copy in table_loads:
        copy.wait()
    q_cos = jnp.concatenate([qbase[:HALF, :]] * (span // LANES), axis=1)
    q_sin = jnp.concatenate([qbase[HALF:, :]] * (span // LANES), axis=1)
    step_cos, step_sin = qstep[:HALF, :], qstep[HALF:, :]
    q_cos, q_sin = q_cos * step_cos - q_sin * step_sin, q_sin * step_cos + q_cos * step_sin
    q_copy(g * 2 + 1 - c, mate).wait_recv()
    q_copy((1 - g) * 2 + 1 - c, mate).wait_recv()

    scale = (NOPE + ROPE) ** (-0.5) * log2e

    @phase
    def _():
        plain = dot_nt(uqt[...], ql[...]) * scale
        turning = dot_nt(urt[...], ql[...]) * scale
        for h in range(heads):
            first = turning[h * ROPE : h * ROPE + HALF, :]
            second = turning[h * ROPE + HALF : (h + 1) * ROPE, :]
            whole = [
                plain[h * NOPE : (h + 1) * NOPE, :],
                first * q_cos - second * q_sin,
                second * q_cos + first * q_sin,
                jnp.zeros((LANES - ROPE, span), F32),
            ]
            whole = jnp.concatenate(whole, axis=0).astype(BF16)
            for n in range(2):
                qt[n, h] = whole[:, n * side : (n + 1) * side]

    def score(slot, h, group):
        key = jnp.concatenate([keys[slot][:, h * NOPE : (h + 1) * NOPE], rots[slot][...]], axis=1)
        return dot(key, qt[group, h])

    def attend(slot, group, first=False, ahead=None):
        ones = jnp.ones((acc.shape[1] - VDIM, span), BF16)
        parts = [[] for _ in range(heads)]
        if ahead is not None:
            todo = head_parts(ahead, 1 - slot)
            for n, part in enumerate(todo):
                parts[max(n - len(todo) + heads, 0)].append(part)
        if first:
            k_pos = lax.broadcasted_iota(jnp.int32, (span, side), 0)
            q_pos = lax.broadcasted_iota(jnp.int32, (span, side), 1) + group * side
            allowed = k_pos <= q_pos

        def weigh(h, scores):
            if first:
                scores = jnp.where(allowed, scores, masked_score)
            new = jnp.max(scores, axis=0, keepdims=True)
            shrink = None
            if not first:
                old = best[h][:1]
                new = jnp.maximum(old, new)
                shrink = jnp.exp2(old - new)
            best[h] = jnp.broadcast_to(new, best.shape[1:])
            return jnp.exp2(scores - new).astype(BF16), shrink

        def gather(h, weights, shrink):
            value = jnp.concatenate([vals[slot][h * VDIM : (h + 1) * VDIM, :], ones], axis=0)
            if first:
                acc[h] = dot(value, weights)
            else:
                acc[h] = acc[h] * shrink + dot(value, weights)

        later = score(slot, 0, group) if first else scored[...]
        weighed = None
        for h in range(heads):
            scores = later
            if h + 1 < heads:
                later = score(slot, h + 1, group)
            elif ahead is not None:
                later = score(1 - slot, 0, group)
            for part in parts[h]:
                part()
            now = weigh(h, scores)
            if weighed is not None:
                gather(h - 1, *weighed)
            weighed = now
        if ahead is not None:
            scored[...] = later
        gather(heads - 1, *weighed)

    def sweep(group, arriving):
        def one(j, slot):
            if arriving:
                early = (i == 0) | ((o < O - 1) & (j >= 2))
                pl.when(early & (j + 2 <= sp))(lambda: relay_in(seq(j + 2)))
                mate_in(seq(j + 1))
            attend(slot, group, ahead=seq(j + 1))
            if arriving:
                pl.when((i == 1) & (o < O - 1) & (j == 1) & (sp >= 3))(lambda: relay_in(seq(3)))
                pl.when((i == 1) & (o == O - 1) & (j + 3 <= sp))(lambda: relay_in(seq(j + 3)))

        @pl.when(sp >= 1)
        def _():
            def two(n):
                one(2 * n + 1, 1)
                one(2 * n + 2, 0)

            each(0, (sp - 1) // 2, two)

            @pl.when(i == 0)
            def _():
                one(sp - 1, 1)
                attend(0, group)

            pl.when(i == 1)(lambda: attend(1, group))

        @phase
        def _():
            for h in range(heads):
                whole = acc[h]
                part = (whole[:VDIM] / whole[VDIM : VDIM + 1]).T.astype(BF16)
                att[pl.ds(pl.multiple_of(group * side, side), side), h * VDIM : (h + 1) * VDIM] = part

    pl.when((o >= 1) & (o == O - 1))(lambda: across_in(1))
    phase(lambda: attend(0, 1 - g, first=True))

    @pl.when((o >= 1) & (o < O - 1))
    def _():
        each(2, o + 1, column_in)
        across_in(1)

    @pl.when((i == 0) & (o >= 1))
    def _():
        mate_in(seq(1))
        kv_heads(seq(1), 1)

    pl.when(sp >= 1)(lambda: scored.__setitem__(..., score(1, 0, 1 - g)))

    @pl.when((o >= 1) & ((i == 0) | (o == O - 1)))
    def _():
        beside_in(1)
        corner_in(1)

    sweep(1 - g, True)

    ow_load.wait()
    width = ow.shape[1] // pieces
    lag = min(5, pieces)

    def pair_copy(second, j):
        return pltpu.make_async_remote_copy(
            src_ref=pair_out.at[second, j],
            dst_ref=pair_in.at[second, j],
            send_sem=pair_send.at[0],
            recv_sem=pair_recv.at[pieces if second else j],
            device_id=mate,
            device_id_type=MESH,
        )

    def cross_copy(j):
        return pltpu.make_async_remote_copy(
            src_ref=cross_out.at[j],
            dst_ref=cross_in.at[j],
            send_sem=cross_send.at[0],
            recv_sem=cross_recv.at[j],
            device_id=across,
            device_id_type=MESH,
        )

    def project(second, group, j):
        top = att[block_rows(group * 2 + 1 - c), :]
        low_part = att[block_rows(group * 2 + c), :]
        part = dot(jnp.concatenate([top, low_part], axis=0), ow[:, j * width : (j + 1) * width])
        pair_out[second, j] = part[:rows].astype(BF16)
        kept[second, j] = part[rows:]
        pair_copy(second, j).start()

    def cross(j):
        pair_copy(0, j).wait_recv()
        cross_out[j] = (kept[0, j] + pair_in[0, j].astype(F32)).astype(BF16)
        cross_copy(j).start()

    @phase
    def _():
        for j in range(pieces):
            project(0, 1 - g, j)
            if j >= lag:
                cross(j - lag)
        for j in range(pieces - lag, pieces):
            cross(j)

    phase(lambda: kv_heads(sp, 0))
    phase(lambda: attend(0, g, first=True))

    @pl.when(sp >= 1)
    def _():
        kv_heads(seq(1), 1)
        scored[...] = score(1, 0, g)

    sweep(g, False)

    @phase
    def _():
        for j in range(pieces):
            project(1, g, j)

    def all_sent(n, copies):
        pltpu.make_async_remote_copy(
            src_ref=n, dst_ref=n, send_sem=copies.at[0], recv_sem=q_recv.at[0], device_id=mate, device_id_type=MESH
        ).wait_send()

    pl.when(i == 0)(lambda: kv_blocks(4, 0, 0).wait_send())
    pl.when(i == 1)(lambda: kv_blocks(5, 0, 0).wait_send())
    pl.when((i == 0) | (o < O - 1))(lambda: kv_blocks(1, 2 * O - 1, 0).wait_send())

    def counted(index, count, counts):
        for n in counts:
            pl.when(count == n)(lambda n=n: kv_blocks(n, index, 0).wait_send())

    def relays_sent(d):
        counted(d, 6 - jnp.where(d == 1, 1, 0) + jnp.where((d == O - 1) & (O >= 4), 1, 0), (5, 6, 7))

    def ups_sent(d):
        skipped = (o == 0) & (d == O - 2) & (O >= 4)
        counted(O + d - 1, 2 + jnp.where(d == 1, 1, 0) - jnp.where(skipped, 1, 0), (1, 2, 3))

    each(1, o + 1, relays_sent)
    each(1, O - o, ups_sent)
    all_sent(ql.at[pl.ds(0, 3 * rows)], q_send)
    all_sent(pair_out, pair_send)
    pltpu.make_async_remote_copy(
        src_ref=pair_out.at[1],
        dst_ref=pair_in.at[1],
        send_sem=pair_send.at[0],
        recv_sem=pair_recv.at[pieces],
        device_id=mate,
        device_id_type=MESH,
    ).wait_recv()
    for j in range(pieces):
        cross_copy(j).wait_recv()
        total = kept[1, j] + pair_in[1, j].astype(F32) + cross_in[j].astype(F32)
        out_ref[:, j * width : (j + 1) * width] = total.astype(BF16)
    all_sent(cross_out, cross_send)


def solution(mesh):
    S, T = mesh.shape["sp"], mesh.shape["tp"]
    assert S % 2 == 0 and T == 4

    def local(tokens, dq, dl, dr, qg, lg, uq, ur, uk, uv, ow):
        rows, depth = tokens.shape
        span = rows * T
        heads = uk.shape[1] // NOPE
        width = ow.shape[1]
        rank = dl.shape[1]
        chunks, pieces = 4, 16
        inverse = np.float32(rope_base) ** (-np.arange(0, ROPE, 2, dtype=np.float32) / np.float32(ROPE))
        inverse = inverse.astype(np.float64)
        tiled = np.tile(inverse, LANES // HALF)

        def both(angles, axis):
            return np.concatenate([np.cos(angles), np.sin(angles)], axis=axis)

        key_base = np.repeat((np.arange(S * T) * rows)[:, None, None] * tiled, 8, axis=1)
        key_step = np.arange(rows)[:, None] * tiled
        query_base = np.repeat((np.arange(S) * span)[:, None, None] * inverse[:, None], LANES, axis=2)
        query_step = inverse[:, None] * np.arange(span)
        tables = [
            jnp.asarray(a, F32) for a in (both(key_base, 1), both(key_step, 0), both(query_base, 1), both(query_step, 0))
        ]
        O = S // 2
        hbm = pl.BlockSpec(memory_space=pl.ANY)
        vmem = pl.BlockSpec(memory_space=pltpu.VMEM)
        dma = lambda n: pltpu.SemaphoreType.DMA((n,))
        like = lambda a: pltpu.VMEM(a.shape, a.dtype)
        operands = [tokens, dq, dl, dr.T, qg.reshape(1, -1), lg.reshape(1, -1), uq, ur, uk, uv, ow, *tables]
        operands = [pltpu.with_memory_space_constraint(a, pltpu.HBM) for a in operands]
        block_height = rows * rank // LANES + rows // 2
        return pl.pallas_call(
            functools.partial(kernel, S, T, chunks, pieces),
            out_shape=jax.ShapeDtypeStruct((rows, width), BF16),
            in_specs=[hbm] * len(operands),
            out_specs=vmem,
            scratch_shapes=[
                *[like(a) for a in operands[:11]],
                pltpu.VMEM((16, LANES), F32),
                pltpu.VMEM((2 * rows, LANES), F32),
                pltpu.VMEM((ROPE, LANES), F32),
                pltpu.VMEM((ROPE, span), F32),
                pltpu.VMEM((S * T, block_height, LANES), BF16),
                pltpu.VMEM((span, dq.shape[1]), BF16),
                pltpu.VMEM((2, heads, NOPE + LANES, span // 2), BF16),
                pltpu.VMEM((heads, VDIM + 16, span // 2), F32),
                pltpu.VMEM((heads, 8, span // 2), F32),
                pltpu.VMEM((span, heads * VDIM), BF16),
                pltpu.VMEM((2, pieces, rows, width // pieces), BF16),
                pltpu.VMEM((2, pieces, rows, width // pieces), BF16),
                pltpu.VMEM((2, pieces, rows, width // pieces), F32),
                pltpu.VMEM((pieces, rows, width // pieces), BF16),
                pltpu.VMEM((pieces, rows, width // pieces), BF16),
                pltpu.VMEM(uq.shape[::-1], BF16),
                pltpu.VMEM(ur.shape[::-1], BF16),
                pltpu.VMEM(uv.shape[::-1], BF16),
                *[
                    pltpu.VMEM((span, heads * NOPE), BF16),
                    pltpu.VMEM((heads * VDIM, span), BF16),
                    pltpu.VMEM((span, LANES), BF16),
                ]
                * 2,
                pltpu.VMEM((span, span // 2), F32),
                dma(2 * chunks + 13),
                dma(2 * O),
                dma(3 * S),
                dma(1),
                dma(T),
                dma(1),
                dma(pieces + 1),
                dma(1),
                dma(pieces),
            ],
            compiler_params=pltpu.CompilerParams(
                collective_id=0, has_side_effects=True, vmem_limit_bytes=46 * 1024 * 1024
            ),
        )(*operands)

    return jax.shard_map(
        local,
        mesh=mesh,
        in_specs=(
            P(("sp", "tp"), None),
            P(),
            P(),
            P(),
            P(),
            P(),
            P(None, "tp"),
            P(None, "tp"),
            P(None, "tp"),
            P(None, "tp"),
            P("tp", None),
        ),
        out_specs=P(("sp", "tp"), None),
        check_vma=False,
    )
```
